512 devices in a mesh: sp: 32 (over z, core), tp: 16 (over y, x).
Axes of the slice: x: 4, y: 4, z: 16, core: 2. Of those that a mesh axis runs over, the one named last changes fastest.
Arguments:
- resid: bfloat16 [6144, 2048], P('sp', 'tp'), may hold values from -12 to 12
- conv_value: bfloat16 [6144, 2048], P('sp', 'tp'), may hold values from -80 to 80
- conv_gate: bfloat16 [6144, 2048], P('sp', 'tp'), may hold values from -6 to 6
- depth_kernel: float32 [31, 2048], P(None, 'tp'), may hold values from -1 to 1
- chan_gain: float32 [2048], P('tp'), may hold values from 0.1 to 1.9
- point_weight: bfloat16 [2048, 2048], P('tp'), may hold values from -0.125 to 0.125
- mix_gain: float32 [2048], replicated, may hold values from 0.1 to 1.9
- out_weight: bfloat16 [2048, 2048], P(None, 'tp'), may hold values from -0.125 to 0.125
- norm_gain: float32 [2048], P('tp'), may hold values from 0.1 to 1.9
- route_ids: int32 [6144, 4], P('sp'), may hold values from 0 to 31, all different within a row; in each aligned block of 192 rows (0 to 191, 192 to 383, ...) at most 32 rows name the same one
- route_weights: float32 [6144, 4], P('sp'), may hold values from 0.05 to 0.5
- gate_experts: bfloat16 [32, 2048, 4096], P('sp', None, 'tp'), may hold values from -0.3125 to 0.3125
- up_experts: bfloat16 [32, 2048, 4096], P('sp', None, 'tp'), may hold values from -0.3125 to 0.3125
- down_experts: bfloat16 [32, 4096, 2048], P('sp', 'tp'), may hold values from -0.09375 to 0.09375
Outputs:
- result: bfloat16 [6144, 2048], P('sp', 'tp')
The draws below stay inside these ranges and needn't reach their ends.
Inputs may be any that keep to these rules, and one draw needn't show every extreme that they name: `route_ids`: each row names 4 different experts; among the 192 rows of one index of sp no expert is named by more than 32 rows, and in some such block an expert is named by exactly 32.
All inputs are finite; a program needn't handle non-finite values.
Results may differ from the reference program's by a relative error of at most 0.024.
Values may be sent and summed in bfloat16 or wider, within the bound.
A program may use at most 64 MiB of HBM per device.

```python
import math
import jax
import jax.numpy as jnp
import numpy as np
from jax import lax

D = 2048
CONV_CH = 2048
F = 4096
E = 32
TOPK = 4
WIDTH = 31
TOK_DEV = 192
TOKENS = 6144
CAP = 32
N_SP = 32
N_TP = 16


def scaled_draw(key, rows, columns, top):
    first, second = jax.random.split(key, 2)
    column_scale = top ** (jnp.arange(columns, dtype=jnp.float32) / columns)
    row_scale = jnp.exp(jax.random.uniform(second, (rows, 1), jnp.float32, -0.69, 0.69))
    base = jax.random.truncated_normal(first, -4.0, 4.0, (rows, columns), jnp.float32)
    return base * column_scale * row_scale


def draw_resid(key, part):
    values = scaled_draw(jax.random.fold_in(key, 11), TOKENS, D, 3.0) * 0.5
    return values.astype(jnp.bfloat16)


def draw_conv_value(key, part):
    values = scaled_draw(jax.random.fold_in(key, 23), TOKENS, CONV_CH, 10.0)
    return values.astype(jnp.bfloat16)


def levels(stream_key, dims, shards, least, high):
    level, own = 1.0, jax.random.fold_in(stream_key, 6)
    for dim, shards_of in shards:
        heights = jnp.exp(jax.random.uniform(jax.random.fold_in(own, dim), (shards_of,), jnp.float32, least / len(shards), high / len(shards)))
        level = level * jnp.repeat(heights, dims[dim] // shards_of).reshape([-1 if axis == dim else 1 for axis in range(len(dims))])
    return level


def assign_block(stream_key, own, number, rows, amount, top, reach, skew):
    order = jax.random.permutation(stream_key, amount)
    crowded, usual = load_shares(amount, rows * top, reach, skew, True), load_shares(amount, rows * top, reach, skew, False)
    places = jnp.arange(amount)

    def named(lengths, turn):
        used = int((lengths > 0).sum())
        fixed = max(1, used // 4)
        shifted = fixed + (places - fixed + turn * (used - fixed)) % max(1, amount - fixed)
        return jnp.zeros((amount,), jnp.int32).at[order[jnp.where(places < fixed, places, shifted)]].set(jnp.asarray(lengths, jnp.int32))

    lengths = jnp.where(number % 4 == 0, named(crowded, number // 4), named(usual, number - number // 4 - 1))
    mixed = jax.random.permutation(jax.random.fold_in(own, 3), amount)
    source_of, receiver = mixed[0:amount // 2 * 2:2], mixed[1:amount // 2 * 2:2]
    margin = jnp.minimum(lengths[source_of] - 1, reach - lengths[receiver]) // 2
    margin = jnp.where((source_of == order[0]) | (receiver == order[0]) | (lengths[receiver] == 0), 0, jnp.maximum(margin, 0))
    shifted = jax.random.randint(jax.random.fold_in(own, 4), (amount // 2,), 0, 1 << 20) % (margin + 1)
    lengths = lengths.at[source_of].add(-shifted).at[receiver].add(shifted)
    members = jnp.searchsorted(jnp.cumsum(lengths), jnp.arange(rows * top), side="right").astype(jnp.int32)
    grid = members.reshape(top, rows).T
    grid = grid[jax.random.permutation(jax.random.fold_in(own, 1), rows)]
    turn = jax.random.randint(jax.random.fold_in(own, 2), (rows, 1), 0, top)
    return jnp.take_along_axis(grid, (jnp.arange(top)[None, :] + turn) % top, axis=1)


def load_shares(amount, total, bound, slope, full):
    weights = [(1 << 20) // math.isqrt(standing ** slope) + 1 for standing in range(1, amount + 1)]
    largest = bound if full else min(bound, max(-(-total // amount), total * weights[0] // sum(weights)))
    least = 1 if total - largest >= amount - 1 else 0
    holding, spare = [largest] + [least] * (amount - 1), total - largest - least * (amount - 1)
    while spare > 0:
        movable = [i for i in range(1, amount) if holding[i] < largest] or [i for i in range(1, amount) if holding[i] < bound]
        pool, left = sum([weights[i] for i in movable]), spare
        for i in movable:
            addition = min(bound - holding[i], max(1, left * weights[i] // pool), spare)
            holding[i] = holding[i] + addition
            spare = spare - addition
    return np.array(holding)


def gaussian(key, extent, scale, most, pieces=(), kind=jnp.bfloat16):
    array = jax.random.normal(key, extent, jnp.float32) * scale
    if len(pieces) > 0:
        array = levels(key, extent, pieces, -0.22, 0.18) * array
    return jnp.clip(array, min=-most, max=most).astype(kind)


def setup_inputs(seed: int = 0) -> dict:
    key_of = jax.random.split(jax.random.key(seed), 15)
    resid = draw_resid(jax.random.fold_in(key_of[14], 71), 0)
    conv_value = draw_conv_value(jax.random.fold_in(key_of[14], 71), 0)
    conv_gate = gaussian(key_of[2], (TOKENS, CONV_CH), 1.5, 6.0, ((0, 32), (1, 16)))
    depth_kernel = gaussian(key_of[3], (WIDTH, CONV_CH), WIDTH ** -0.5, 1.0, ((1, 16),), jnp.float32)
    chan_gain = jnp.clip(1.0 + 0.18 * jax.random.normal(key_of[4], (CONV_CH,), jnp.float32), 0.1, 1.9)
    point_weight = gaussian(key_of[5], (CONV_CH, CONV_CH), CONV_CH ** -0.5, 0.125, ((0, 16),))
    mix_gain = jnp.clip(1.0 + 0.18 * jax.random.normal(key_of[6], (CONV_CH,), jnp.float32), 0.1, 1.9)
    out_weight = gaussian(key_of[7], (CONV_CH, D), CONV_CH ** -0.5, 0.125, ((1, 16),))
    norm_gain = jnp.clip(1.0 + 0.18 * jax.random.normal(key_of[8], (D,), jnp.float32), 0.1, 1.9)
    route_ids_keys = jax.random.split(jax.random.fold_in(key_of[9], 1), TOKENS // TOK_DEV)
    route_ids_turns = jax.random.permutation(jax.random.fold_in(key_of[9], 3), TOKENS // TOK_DEV)
    route_ids = jax.vmap(lambda own, number: assign_block(jax.random.fold_in(key_of[9], 2), own, number, TOK_DEV, E, TOPK, CAP, 2))(route_ids_keys, route_ids_turns).reshape((TOKENS, TOPK))
    route_weights = jnp.clip(0.05 + 0.45 * jax.random.uniform(key_of[10], (TOKENS, TOPK), jnp.float32) ** levels(key_of[10], (TOKENS, TOPK), ((0, 32),), -0.2, 0.2), 0.05, 0.5)
    gate_experts = gaussian(key_of[11], (E, D, F), (D // 6) ** -0.5, 0.3125, ((0, 32), (2, 16)))
    up_experts = gaussian(key_of[12], (E, D, F), (D // 6) ** -0.5, 0.3125, ((0, 32), (2, 16)))
    down_experts = gaussian(key_of[13], (E, F, D), F ** -0.5, 0.09375, ((0, 32), (1, 16)))
    return dict(resid=resid, conv_value=conv_value, conv_gate=conv_gate, depth_kernel=depth_kernel, chan_gain=chan_gain, point_weight=point_weight, mix_gain=mix_gain, out_weight=out_weight, norm_gain=norm_gain, route_ids=route_ids, route_weights=route_weights, gate_experts=gate_experts, up_experts=up_experts, down_experts=down_experts)


epsilon = 1e-05
clamp_limit = 7.0
swish_slope = 1.702

def rounded_sum(left, right, blocks):
    inner = left.shape[1] // blocks
    total = jnp.zeros((left.shape[0], right.shape[1]), jnp.float32)
    for block in range(blocks):
        part = jnp.dot(left[:, block * inner:(block + 1) * inner], right[block * inner:(block + 1) * inner], preferred_element_type=jnp.float32)
        total = total + lax.optimization_barrier(part.astype(jnp.bfloat16)).astype(jnp.float32)
    return total

def reference(resid, conv_value, conv_gate, depth_kernel, chan_gain, point_weight, mix_gain, out_weight, norm_gain, route_ids, route_weights, gate_experts, up_experts, down_experts):
    gated = (conv_value.astype(jnp.float32) * jax.nn.sigmoid(conv_gate.astype(jnp.float32))).astype(jnp.bfloat16)
    padded = jnp.concatenate([jnp.zeros((WIDTH - 1, CONV_CH), jnp.bfloat16), gated], axis=0)
    conv = jnp.zeros((TOKENS, CONV_CH), jnp.float32)
    for tap in range(WIDTH):
        conv = conv + padded[tap:tap + TOKENS].astype(jnp.float32) * depth_kernel[tap]
    center = conv - lax.optimization_barrier(jnp.mean(conv, axis=1, keepdims=True))
    spread = lax.optimization_barrier(jnp.mean(center * center, axis=1, keepdims=True))
    act = jax.nn.silu(center * lax.rsqrt(spread + epsilon) * chan_gain).astype(jnp.bfloat16)
    point = rounded_sum(act, point_weight, N_TP)
    mixed = (point * lax.rsqrt(lax.optimization_barrier(jnp.mean(point * point, axis=1, keepdims=True)) + epsilon) * mix_gain).astype(jnp.bfloat16)
    middle = (resid.astype(jnp.float32) + jnp.dot(mixed, out_weight, preferred_element_type=jnp.float32)).astype(jnp.bfloat16)
    middle32 = middle.astype(jnp.float32)
    normed = (middle32 * lax.rsqrt(lax.optimization_barrier(jnp.mean(middle32 * middle32, axis=1, keepdims=True)) + epsilon) * norm_gain).astype(jnp.bfloat16)
    flat_ids = route_ids.reshape(-1).astype(jnp.int32)
    flat_weights = route_weights.reshape(-1)
    routed = TOKENS * TOPK
    total = jnp.zeros((TOKENS, D), jnp.float32)
    for expert in range(E):
        found = jnp.nonzero(flat_ids == expert, size=N_SP * CAP, fill_value=routed)[0].astype(jnp.int32)
        valid = found < routed
        token = jnp.minimum(found // TOPK, TOKENS - 1).astype(jnp.int32)
        weight = jnp.where(valid, flat_weights[jnp.minimum(found, routed - 1)], 0.0)
        rows = normed[token]
        gate_pre = jnp.minimum(jnp.dot(rows, gate_experts[expert], preferred_element_type=jnp.float32), clamp_limit)
        up_pre = jnp.clip(jnp.dot(rows, up_experts[expert], preferred_element_type=jnp.float32), -clamp_limit, clamp_limit)
        hidden = (gate_pre * jax.nn.sigmoid(swish_slope * gate_pre) * (up_pre + 1.0)).astype(jnp.bfloat16)
        expert_out = rounded_sum(hidden, down_experts[expert], N_TP).astype(jnp.bfloat16)
        total = total.at[token].add(expert_out.astype(jnp.float32) * weight[:, None])
    return (middle32 + total).astype(jnp.bfloat16)
```

```python
import jax
import jax.numpy as jnp
from jax import lax
from jax.experimental import pallas as pl
from jax.experimental.pallas import tpu as pltpu
from jax.sharding import Mesh
from jax.sharding import PartitionSpec as P

E = 32
TOPK = 4
CAP = 32
TP = ("tp_0", "tp_1")
MESH = pl.DeviceIdType.MESH

epsilon = 1e-05
clamp_limit = 7.0
swish_slope = 1.702

SIDE = 4
CHIPS = 16
LANES = 128
ROWS = E * CAP
CHUNKS = 4
CROWS = ROWS // CHUNKS
PERCHUNK = CROWS // CAP
OFFSETS = [0, 1, -1, 2, -2, 3, -3, 4, -4, 5, -5, 6, -6, 7, -7, 8]


class Plane:
    def __init__(self, y, x):
        self.pos = (y, x)
        self.axes = ("tp_0", "tp_1")

    def neighbour(self, dim, step):
        return {self.axes[dim]: lax.rem(self.pos[dim] + step + SIDE, SIDE)}

    def at(self, dim, step):
        return lax.rem(self.pos[dim] + step + SIDE, SIDE)

    def line(self, ref, dim, index, rows):
        if dim == 0:
            return ref.at[index, :, rows, :]
        return ref.at[:, index, rows, :]

    def one(self, ref, dim, index, rows):
        if dim == 0:
            return ref.at[index, self.pos[1], rows, :]
        return ref.at[self.pos[0], index, rows, :]


def copy_to(src, dst, send, recv, device):
    return pltpu.make_async_remote_copy(
        src_ref=src, dst_ref=dst, send_sem=send, recv_sem=recv, device_id=device, device_id_type=MESH
    )


class Gather:
    def __init__(self, plane, buf, base, count, send, recv, chunk):
        self.plane, self.buf, self.chunk = plane, buf, chunk
        self.send, self.recv = send, recv
        self.half = count // 2
        self.quarter = count // 4
        self.base = base
        self.pending = {}

    def rows(self, color):
        start = self.base + color * self.half
        return pl.ds(start, self.half)

    def part(self, color, which):
        start = self.base + color * self.half + which * self.quarter
        return pl.ds(start, self.quarter)

    def go(self, color, step, way, src, dst, device):
        sem = (self.chunk, color, step, way)
        op = copy_to(src, dst, self.send.at[sem], self.recv.at[sem], device)
        op.start()
        self.pending[(color, step, way)] = op

    def issue(self, step):
        plane = self.plane
        for color in range(2):
            near = 1 - color
            far = color
            dim = near if step < 2 else far
            view = plane.one if step < 2 else plane.line
            ahead, behind = plane.neighbour(dim, 1), plane.neighbour(dim, -1)
            if step % 2 == 0:
                block = view(self.buf, dim, plane.pos[dim], self.rows(color))
                self.go(color, step, 0, block, block, ahead)
                self.go(color, step, 1, block, block, behind)
            else:
                self.pending[(color, step - 1, 0)].wait_recv()
                block = view(self.buf, dim, plane.at(dim, -1), self.part(color, 0))
                self.go(color, step, 0, block, block, ahead)
                self.pending[(color, step - 1, 1)].wait_recv()
                block = view(self.buf, dim, plane.at(dim, 1), self.part(color, 1))
                self.go(color, step, 1, block, block, behind)

    def arrived(self, step):
        for color in range(2):
            for way in range(2):
                self.pending[(color, step, way)].wait_recv()

    def sent(self):
        for op in self.pending.values():
            op.wait_send()


class Reduce:
    def __init__(self, plane, buf, base, count, lands, send, recv, chunk):
        self.plane, self.buf, self.chunk = plane, buf, chunk
        self.send, self.recv = send, recv
        self.half = count // 2
        self.quarter = count // 4
        self.base = base
        self.lands = lands
        self.pending = {}

    def rows(self, color):
        return pl.ds(self.base + color * self.half, self.half)

    def part(self, color, which):
        return pl.ds(self.base + color * self.half + which * self.quarter, self.quarter)

    def go(self, color, step, way, src, device):
        sem = (self.chunk, color, step, way)
        dst = self.lands[step].at[self.chunk, color, way]
        op = copy_to(src, dst, self.send.at[sem], self.recv.at[sem], device)
        op.start()
        self.pending[(color, step, way)] = op

    def land(self, color, step, way):
        self.pending[(color, step, way)].wait_recv()
        return self.lands[step].at[self.chunk, color, way]

    def issue(self, step):
        plane = self.plane
        for color in range(2):
            near = 1 - color
            far = color
            dim = far if step < 2 else near
            view = plane.line if step < 2 else plane.one
            ahead, behind = plane.neighbour(dim, 1), plane.neighbour(dim, -1)
            if step == 2:
                self.fold(color)
            if step % 2 == 0:
                opposite = plane.at(dim, 2)
                self.go(color, step, 0, view(self.buf, dim, opposite, self.part(color, 0)), ahead)
                self.go(color, step, 1, view(self.buf, dim, opposite, self.part(color, 1)), behind)
            else:
                for way, (shift, device) in enumerate(((1, ahead), (-1, behind))):
                    landed = self.land(color, step - 1, way)
                    target = view(self.buf, dim, plane.at(dim, shift), self.part(color, way))
                    target[...] = (target[...].astype(jnp.float32) + landed[...].astype(jnp.float32)).astype(
                        jnp.bfloat16
                    )
                    whole = view(self.buf, dim, plane.at(dim, shift), self.rows(color))
                    self.go(color, step, way, whole, device)

    def fold(self, color):
        plane = self.plane
        far = color
        own = plane.line(self.buf, far, plane.pos[far], self.rows(color))
        first, second = self.land(color, 1, 0), self.land(color, 1, 1)
        own[...] = (
            own[...].astype(jnp.float32) + first[...].astype(jnp.float32) + second[...].astype(jnp.float32)
        ).astype(jnp.bfloat16)

    def total(self, color):
        plane = self.plane
        near = 1 - color
        own = plane.one(self.buf, near, plane.pos[near], self.rows(color))
        first, second = self.land(color, 3, 0), self.land(color, 3, 1)
        return own[...].astype(jnp.float32) + first[...].astype(jnp.float32) + second[...].astype(jnp.float32)

    def sent(self):
        for op in self.pending.values():
            op.wait_send()


def land_shapes(chunks, count):
    half, quarter = count // 2, count // 4
    return [
        pltpu.VMEM((chunks, 2, 2, SIDE, quarter, LANES), jnp.bfloat16),
        pltpu.VMEM((chunks, 2, 2, SIDE, half, LANES), jnp.bfloat16),
        pltpu.VMEM((chunks, 2, 2, quarter, LANES), jnp.bfloat16),
        pltpu.VMEM((chunks, 2, 2, half, LANES), jnp.bfloat16),
    ]


def expert_kernel(
    outgoing,
    middle,
    mix_hi,
    mix_lo,
    gain,
    gate_hbm,
    up_hbm,
    down_hbm,
    result,
    gate,
    up,
    down,
    rows,
    normed,
    partial,
    land0,
    land1,
    land2,
    land3,
    total,
    back,
    weight_sem,
    ag_send,
    ag_recv,
    rs_send,
    rs_recv,
    out_send,
    out_recv,
    back_send,
    back_recv,
):
    sp = lax.axis_index("sp")
    y, x = lax.axis_index("tp_0"), lax.axis_index("tp_1")
    z, core = sp // 2, lax.rem(sp, 2)
    plane = Plane(y, x)

    barrier = pltpu.get_barrier_semaphore()

    @pl.loop(1, E)
    def _(d):
        pl.semaphore_signal(barrier, inc=1, device_id={"sp": lax.rem(sp + d, E)}, device_id_type=MESH)

    for dim in range(2):
        for step in (1, -1):
            pl.semaphore_signal(barrier, inc=1, device_id=plane.neighbour(dim, step), device_id_type=MESH)

    fetches = [
        pltpu.make_async_copy(src.at[0], dst, weight_sem.at[i])
        for i, (src, dst) in enumerate(((gate_hbm, gate), (up_hbm, up), (down_hbm, down)))
    ]
    for fetch in fetches:
        fetch.start()
    pl.semaphore_wait(barrier, E - 1 + 4)

    other = 1 - core
    for i, offset in enumerate(OFFSETS):
        chip = lax.rem(z - offset + CHIPS, CHIPS)
        place = pl.ds(pl.multiple_of((2 * i + core) * CAP, CAP), CAP)
        for way in range(2):
            if i == 0 and way == 1:
                continue
            target = 2 * chip + (other if i == 0 else way)
            copy_to(
                outgoing.at[target],
                rows.at[y, x, place, :],
                out_send,
                out_recv.at[2 * i // PERCHUNK],
                {"sp": target},
            ).start()
    own_place = pl.ds(pl.multiple_of(core * CAP, CAP), CAP)
    rows[y, x, own_place, :] = outgoing[sp]

    gathers = [Gather(plane, rows, c * CROWS, CROWS, ag_send, ag_recv, c) for c in range(CHUNKS)]
    lands = (land0, land1, land2, land3)
    reduces = [Reduce(plane, partial, c * CROWS, CROWS, lands, rs_send, rs_recv, c) for c in range(CHUNKS)]

    def begin(c):
        count = CROWS - (CAP if c == 0 else 0)
        landed = rows.at[y, x, pl.ds(c * CROWS, count), :]
        copy_to(landed, landed, out_send, out_recv.at[c], {"sp": sp}).wait_recv()
        gathers[c].issue(0)

    def compute(c):
        gathers[c].arrived(3)
        if c == 0:
            for fetch in fetches:
                fetch.wait()
        step = 32

        @pl.loop(0, CROWS // step)
        def _(i):
            at = pl.multiple_of(i * step, step)
            block = rows[:, :, pl.ds(c * CROWS + at, step), :].astype(jnp.float32)
            block = block.reshape(SIDE * SIDE, step, LANES)
            squares = jnp.sum(jnp.sum(block * block, axis=0), axis=1, keepdims=True)
            scale = lax.rsqrt(squares / (SIDE * SIDE * LANES) + epsilon)
            scaled = block * scale[None] * gain[...][:, None, :]
            normed[:, pl.ds(at, step), :] = scaled.astype(jnp.bfloat16)

        left = jnp.concatenate([normed[b] for b in range(SIDE * SIDE)], axis=1)
        gate_pre = jnp.minimum(jnp.dot(left, gate[...], preferred_element_type=jnp.float32), clamp_limit)
        up_pre = jnp.clip(
            jnp.dot(left, up[...], preferred_element_type=jnp.float32), -clamp_limit, clamp_limit
        )
        hidden = (gate_pre * jax.nn.sigmoid(swish_slope * gate_pre) * (up_pre + 1.0)).astype(jnp.bfloat16)
        place = pl.ds(c * CROWS, CROWS)
        for j in range(SIDE * SIDE // 2):
            both = jnp.dot(
                hidden, down[:, 2 * j * LANES : 2 * (j + 1) * LANES], preferred_element_type=jnp.float32
            ).astype(jnp.bfloat16)
            for k in range(2):
                b = 2 * j + k
                partial[b // SIDE, b % SIDE, place, :] = both[:, k * LANES : (k + 1) * LANES]
        reduces[c].issue(0)

    def finish(c):
        half = CROWS // 2
        for color in range(2):
            total[pl.ds(c * CROWS + color * half, half), :] = reduces[c].total(color).astype(jnp.bfloat16)
        for p in range(c * PERCHUNK, (c + 1) * PERCHUNK):
            i, way = p // 2, p % 2
            if i == 0 and way == 1:
                continue
            chip = lax.rem(z + OFFSETS[i] + CHIPS, CHIPS)
            if i == 0:
                target = 2 * chip + other
                src = total.at[pl.ds(pl.multiple_of(other * CAP, CAP), CAP), :]
            else:
                target = 2 * chip + way
                src = total.at[pl.ds(p * CAP, CAP), :]
            copy_to(src, back.at[sp], back_send, back_recv, {"sp": target}).start()
        if c == 0:
            back[sp] = total[own_place, :]

    stages = [
        begin,
        lambda c: gathers[c].issue(1),
        lambda c: (gathers[c].arrived(1), gathers[c].issue(2)),
        lambda c: gathers[c].issue(3),
        compute,
        lambda c: reduces[c].issue(1),
        lambda c: reduces[c].issue(2),
        lambda c: reduces[c].issue(3),
        finish,
    ]
    for slot in range(CHUNKS + len(stages) - 1):
        for stage in (0, 1, 2, 3, 5, 6, 7, 8, 4):
            c = slot - stage
            if 0 <= c < CHUNKS:
                stages[stage](c)

    whole = back.at[pl.ds(0, E - 1)]
    copy_to(whole, whole, back_send, back_recv, {"sp": sp}).wait_recv()
    values = back[...].reshape(ROWS, LANES)
    routed = jnp.dot(mix_hi[...], values, preferred_element_type=jnp.float32)
    routed = routed + jnp.dot(mix_lo[...], values, preferred_element_type=jnp.float32)
    result[...] = (middle[...].astype(jnp.float32) + routed).astype(jnp.bfloat16)

    sent = outgoing.at[pl.ds(0, E - 1)]
    copy_to(sent, sent, out_send, out_recv.at[0], {"sp": sp}).wait_send()
    sent = total.at[pl.ds(0, ROWS - CAP), :]
    copy_to(sent, sent, back_send, back_recv, {"sp": sp}).wait_send()
    for c in range(CHUNKS):
        gathers[c].sent()
        reduces[c].sent()


def experts(outgoing, middle, mix_hi, mix_lo, gain, gate_experts, up_experts, down_experts):
    vmem = pl.BlockSpec(memory_space=pltpu.VMEM)
    hbm = pl.BlockSpec(memory_space=pl.ANY)
    bf16 = jnp.bfloat16
    depth, hidden = gate_experts.shape[1], gate_experts.shape[2]
    sems = pltpu.SemaphoreType.DMA((CHUNKS, 2, 4, 2))
    one = pltpu.SemaphoreType.DMA
    return pl.pallas_call(
        expert_kernel,
        out_shape=jax.ShapeDtypeStruct(middle.shape, bf16),
        in_specs=[vmem] * 5 + [hbm] * 3,
        out_specs=vmem,
        scratch_shapes=[
            pltpu.VMEM((depth, hidden), bf16),
            pltpu.VMEM((depth, hidden), bf16),
            pltpu.VMEM((hidden, depth), bf16),
            pltpu.VMEM((SIDE, SIDE, ROWS, LANES), bf16),
            pltpu.VMEM((SIDE * SIDE, CROWS, LANES), bf16),
            pltpu.VMEM((SIDE, SIDE, ROWS, LANES), bf16),
            *land_shapes(CHUNKS, CROWS),
            pltpu.VMEM((ROWS, LANES), bf16),
            pltpu.VMEM((E, CAP, LANES), bf16),
            one((3,)),
            sems,
            sems,
            sems,
            sems,
            one,
            one((CHUNKS,)),
            one,
            one,
        ],
        compiler_params=pltpu.CompilerParams(
            collective_id=1, has_side_effects=True, vmem_limit_bytes=48 * 1024 * 1024
        ),
        name="experts",
    )(outgoing, middle, mix_hi, mix_lo, gain, gate_experts, up_experts, down_experts)


def from_behind(block, axis, distance):
    devices = range(lax.axis_size(axis))
    route = [(i - distance, i) for i in devices if i - distance in devices]
    return lax.ppermute(block, axis, route)


def over_axes(value, axes):
    for axis in axes:
        value = lax.psum(value, axis)
    return value


def split_up(value, dim, count):
    dims = value.shape
    pieces = value.reshape(*dims[:dim], count, dims[dim] // count, *dims[dim + 1 :])
    return jnp.moveaxis(pieces, dim, 0)


def summed_on_arrival(value, axis, dim):
    pieces = split_up(value, dim, lax.axis_size(axis))
    arrived = lax.all_to_all(pieces, axis, split_axis=0, concat_axis=0, tiled=True)
    return arrived.astype(jnp.float32).sum(axis=0)


def from_everyone(value, axis):
    copies = jnp.broadcast_to(value, (lax.axis_size(axis), *value.shape))
    return lax.all_to_all(copies, axis, split_axis=0, concat_axis=0, tiled=True)


def laid_out(pieces, dim):
    dims = list(pieces.shape[1:])
    dims[dim] *= pieces.shape[0]
    return jnp.moveaxis(pieces, 0, dim).reshape(dims)


def gathered_copies(value, axis, dim):
    pieces = from_everyone(value, axis)
    return laid_out(pieces, dim)


def shards(
    resid,
    conv_value,
    conv_gate,
    depth_kernel,
    chan_gain,
    point_weight,
    mix_gain,
    out_weight,
    norm_gain,
    route_ids,
    route_weights,
    gate_experts,
    up_experts,
    down_experts,
):
    tok_rows, chan_local = conv_value.shape
    feat_local = resid.shape[1]
    lookback = depth_kernel.shape[0] - 1
    gated = (conv_value.astype(jnp.float32) * jax.nn.sigmoid(conv_gate.astype(jnp.float32))).astype(
        jnp.bfloat16
    )
    earlier = from_behind(gated[tok_rows - lookback :], "sp", 1)
    padded = jnp.concatenate([earlier, gated], axis=0)
    conv = jnp.zeros((tok_rows, chan_local), jnp.float32)
    for tap in range(lookback + 1):
        conv = conv + padded[tap : tap + tok_rows].astype(jnp.float32) * depth_kernel[tap]
    chan_total = chan_local * lax.axis_size(TP)
    row_sums, row_squares = (
        over_axes(jnp.sum(conv, axis=1), TP),
        over_axes(jnp.sum(conv * conv, axis=1), TP),
    )
    row_mean = row_sums / chan_total
    row_var = row_squares / chan_total - row_mean * row_mean
    act = jax.nn.silu(
        (conv - row_mean[:, None]) * lax.rsqrt(row_var[:, None] + epsilon) * chan_gain
    ).astype(jnp.bfloat16)
    point = summed_on_arrival(
        jnp.dot(act, point_weight, preferred_element_type=jnp.float32).astype(jnp.bfloat16), TP, 0
    )
    mixed = (
        point * lax.rsqrt(jnp.mean(point * point, axis=1, keepdims=True) + epsilon) * mix_gain
    ).astype(jnp.bfloat16)
    branch = jnp.dot(gathered_copies(mixed, TP, 0), out_weight, preferred_element_type=jnp.float32)
    middle = (resid.astype(jnp.float32) + branch).astype(jnp.bfloat16)
    gain = from_everyone(norm_gain, TP).reshape(SIDE * SIDE, LANES)

    flat_ids = route_ids.reshape(-1)
    expert_table = (flat_ids[:, None] == jnp.arange(E, dtype=jnp.int32)[None, :]).astype(jnp.int32)
    earlier_count = jnp.cumsum(expert_table, axis=0) - expert_table
    position = jnp.sum(earlier_count * expert_table, axis=1)
    slot_grid = (flat_ids * CAP + position).reshape(tok_rows, TOPK)
    hits = slot_grid[None, :, :] == jnp.arange(E * CAP, dtype=jnp.int32)[:, None, None]
    picker = jnp.any(hits, axis=2).astype(jnp.bfloat16)
    outgoing = (
        jnp.dot(picker, middle, preferred_element_type=jnp.float32)
        .astype(jnp.bfloat16)
        .reshape(E, CAP, feat_local)
    )
    back_hits = slot_grid[:, :, None] == jnp.arange(E * CAP, dtype=jnp.int32)[None, None, :]
    mixer = jnp.sum(jnp.where(back_hits, route_weights[:, :, None], 0.0), axis=1)
    mix_hi = lax.reduce_precision(mixer, 8, 7)
    mix_lo = (mixer - mix_hi).astype(jnp.bfloat16)
    return experts(
        outgoing, middle, mix_hi.astype(jnp.bfloat16), mix_lo, gain, gate_experts, up_experts, down_experts
    )


def solution(mesh):
    split = Mesh(mesh.devices.reshape(mesh.shape["sp"], 4, 4), ("sp", "tp_0", "tp_1"))
    return jax.shard_map(
        shards,
        mesh=split,
        in_specs=(
            P("sp", TP),
            P("sp", TP),
            P("sp", TP),
            P(None, TP),
            P(TP),
            P(TP, None),
            P(),
            P(None, TP),
            P(TP),
            P("sp", None),
            P("sp", None),
            P("sp", None, TP),
            P("sp", None, TP),
            P("sp", TP, None),
        ),
        out_specs=P("sp", TP),
        check_vma=False,
    )
```

```python
import jax
import jax.numpy as jnp
from jax import lax
from jax.experimental import pallas as pl
from jax.experimental.pallas import tpu as pltpu
from jax.sharding import Mesh
from jax.sharding import PartitionSpec as P

E = 32
TOPK = 4
CAP = 32
TP = ("tp_0", "tp_1")
MESH = pl.DeviceIdType.MESH

epsilon = 1e-05
clamp_limit = 7.0
swish_slope = 1.702

SIDE = 4
CHIPS = 16
LANES = 128
ROWS = E * CAP
CHUNKS = 4
CROWS = ROWS // CHUNKS
PERCHUNK = CROWS // CAP
OFFSETS = [0, 1, -1, 2, -2, 3, -3, 4, -4, 5, -5, 6, -6, 7, -7, 8]


class Plane:
    def __init__(self, y, x):
        self.pos = (y, x)
        self.axes = ("tp_0", "tp_1")

    def neighbour(self, dim, step):
        return {self.axes[dim]: lax.rem(self.pos[dim] + step + SIDE, SIDE)}

    def at(self, dim, step):
        return lax.rem(self.pos[dim] + step + SIDE, SIDE)

    def line(self, ref, dim, index, rows):
        if dim == 0:
            return ref.at[index, :, rows, :]
        return ref.at[:, index, rows, :]

    def one(self, ref, dim, index, rows):
        if dim == 0:
            return ref.at[index, self.pos[1], rows, :]
        return ref.at[self.pos[0], index, rows, :]


def copy_to(src, dst, send, recv, device):
    return pltpu.make_async_remote_copy(
        src_ref=src, dst_ref=dst, send_sem=send, recv_sem=recv, device_id=device, device_id_type=MESH
    )


class Gather:
    def __init__(self, plane, buf, base, count, send, recv, chunk):
        self.plane, self.buf, self.chunk = plane, buf, chunk
        self.send, self.recv = send, recv
        self.half = count // 2
        self.quarter = count // 4
        self.base = base
        self.pending = {}

    def rows(self, color):
        start = self.base + color * self.half
        return pl.ds(start, self.half)

    def part(self, color, which):
        start = self.base + color * self.half + which * self.quarter
        return pl.ds(start, self.quarter)

    def go(self, color, step, way, src, dst, device):
        sem = (self.chunk, color, step, way)
        op = copy_to(src, dst, self.send.at[sem], self.recv.at[sem], device)
        op.start()
        self.pending[(color, step, way)] = op

    def issue(self, step):
        plane = self.plane
        for color in range(2):
            near = 1 - color
            far = color
            dim = near if step < 2 else far
            view = plane.one if step < 2 else plane.line
            ahead, behind = plane.neighbour(dim, 1), plane.neighbour(dim, -1)
            if step % 2 == 0:
                block = view(self.buf, dim, plane.pos[dim], self.rows(color))
                self.go(color, step, 0, block, block, ahead)
                self.go(color, step, 1, block, block, behind)
            else:
                self.pending[(color, step - 1, 0)].wait_recv()
                block = view(self.buf, dim, plane.at(dim, -1), self.part(color, 0))
                self.go(color, step, 0, block, block, ahead)
                self.pending[(color, step - 1, 1)].wait_recv()
                block = view(self.buf, dim, plane.at(dim, 1), self.part(color, 1))
                self.go(color, step, 1, block, block, behind)

    def arrived(self, step):
        for color in range(2):
            for way in range(2):
                self.pending[(color, step, way)].wait_recv()

    def sent(self):
        for op in self.pending.values():
            op.wait_send()


class Reduce:
    def __init__(self, plane, buf, base, count, lands, send, recv, chunk):
        self.plane, self.buf, self.chunk = plane, buf, chunk
        self.send, self.recv = send, recv
        self.half = count // 2
        self.quarter = count // 4
        self.base = base
        self.lands = lands
        self.pending = {}

    def rows(self, color):
        return pl.ds(self.base + color * self.half, self.half)

    def part(self, color, which):
        return pl.ds(self.base + color * self.half + which * self.quarter, self.quarter)

    def go(self, color, step, way, src, device):
        sem = (self.chunk, color, step, way)
        dst = self.lands[step].at[self.chunk, color, way]
        op = copy_to(src, dst, self.send.at[sem], self.recv.at[sem], device)
        op.start()
        self.pending[(color, step, way)] = op

    def land(self, color, step, way):
        self.pending[(color, step, way)].wait_recv()
        return self.lands[step].at[self.chunk, color, way]

    def issue(self, step):
        plane = self.plane
        for color in range(2):
            near = 1 - color
            far = color
            dim = far if step < 2 else near
            view = plane.line if step < 2 else plane.one
            ahead, behind = plane.neighbour(dim, 1), plane.neighbour(dim, -1)
            if step == 2:
                self.fold(color)
            if step % 2 == 0:
                opposite = plane.at(dim, 2)
                self.go(color, step, 0, view(self.buf, dim, opposite, self.part(color, 0)), ahead)
                self.go(color, step, 1, view(self.buf, dim, opposite, self.part(color, 1)), behind)
            else:
                for way, (shift, device) in enumerate(((1, ahead), (-1, behind))):
                    landed = self.land(color, step - 1, way)
                    target = view(self.buf, dim, plane.at(dim, shift), self.part(color, way))
                    target[...] = (target[...].astype(jnp.float32) + landed[...].astype(jnp.float32)).astype(
                        jnp.bfloat16
                    )
                    whole = view(self.buf, dim, plane.at(dim, shift), self.rows(color))
                    self.go(color, step, way, whole, device)

    def fold(self, color):
        plane = self.plane
        far = color
        own = plane.line(self.buf, far, plane.pos[far], self.rows(color))
        first, second = self.land(color, 1, 0), self.land(color, 1, 1)
        own[...] = (
            own[...].astype(jnp.float32) + first[...].astype(jnp.float32) + second[...].astype(jnp.float32)
        ).astype(jnp.bfloat16)

    def total(self, color):
        plane = self.plane
        near = 1 - color
        own = plane.one(self.buf, near, plane.pos[near], self.rows(color))
        first, second = self.land(color, 3, 0), self.land(color, 3, 1)
        return own[...].astype(jnp.float32) + first[...].astype(jnp.float32) + second[...].astype(jnp.float32)

    def sent(self):
        for op in self.pending.values():
            op.wait_send()


MIX_CHUNKS = 1
TOK = 192
HALO = 32
PAD_TOK = 256
TAPS = 31
WIDE = SIDE * SIDE * LANES


def land_shapes(chunks, count):
    half, quarter = count // 2, count // 4
    return [
        pltpu.VMEM((chunks, 2, 2, SIDE, quarter, LANES), jnp.bfloat16),
        pltpu.VMEM((chunks, 2, 2, SIDE, half, LANES), jnp.bfloat16),
        pltpu.VMEM((chunks, 2, 2, quarter, LANES), jnp.bfloat16),
        pltpu.VMEM((chunks, 2, 2, half, LANES), jnp.bfloat16),
    ]


def iota(shape, dim):
    return lax.broadcasted_iota(jnp.int32, shape, dim)


def layer_kernel(
    value_hbm,
    gating_hbm,
    taps_hbm,
    resid_hbm,
    point_hbm,
    outw_hbm,
    gate_hbm,
    up_hbm,
    down_hbm,
    chan_gain,
    mix_gain,
    norm_gain,
    routes,
    result,
    value,
    gating,
    taps,
    resid,
    pointw,
    outw,
    gate,
    up,
    down,
    padded,
    halo,
    conv,
    message,
    stats,
    gains,
    scaled_out,
    picker,
    mixer_hi,
    mixer_lo,
    mid,
    outgoing,
    mix_part,
    mix_rows,
    mland0,
    mland1,
    mland2,
    mland3,
    rows,
    normed,
    partial,
    land0,
    land1,
    land2,
    land3,
    total,
    back,
    fetch_sem,
    halo_send,
    halo_recv,
    stat_send,
    stat_recv,
    mag_send,
    mag_recv,
    mrs_send,
    mrs_recv,
    ag_send,
    ag_recv,
    rs_send,
    rs_recv,
    out_send,
    out_recv,
    back_send,
    back_recv,
):
    f32, bf16 = jnp.float32, jnp.bfloat16
    sp = lax.axis_index("sp")
    y, x = lax.axis_index("tp_0"), lax.axis_index("tp_1")
    z, core = sp // 2, lax.rem(sp, 2)
    plane = Plane(y, x)

    barrier = pltpu.get_barrier_semaphore()

    @pl.loop(1, E)
    def _(d):
        pl.semaphore_signal(barrier, inc=1, device_id={"sp": lax.rem(sp + d, E)}, device_id_type=MESH)

    mates = []
    for dy in range(SIDE):
        for dx in range(SIDE):
            if dy or dx:
                mates.append({"tp_0": lax.rem(y + dy, SIDE), "tp_1": lax.rem(x + dx, SIDE)})
    for mate in mates:
        pl.semaphore_signal(barrier, inc=1, device_id=mate, device_id_type=MESH)

    fetches = []
    for i, (src, dst) in enumerate(
        (
            (value_hbm, value),
            (gating_hbm, gating),
            (taps_hbm, taps),
            (point_hbm, pointw),
            (outw_hbm, outw),
            (resid_hbm, resid),
            (gate_hbm.at[0], gate),
            (up_hbm.at[0], up),
            (down_hbm.at[0], down),
        )
    ):
        fetch = pltpu.make_async_copy(src, dst, fetch_sem.at[i])
        fetch.start()
        fetches.append(fetch)

    for i in range(3):
        fetches[i].wait()
    unit = value[...].astype(f32) * jax.nn.sigmoid(gating[...].astype(f32))
    padded[HALO:, :] = unit.astype(bf16).astype(f32)

    def convolve(first, count):
        acc = jnp.zeros((count, LANES), f32)
        for tap in range(TAPS):
            start = first + HALO - (TAPS - 1) + tap
            acc = acc + padded[start : start + count, :] * taps[tap : tap + 1, :]
        return acc

    conv[HALO:, :] = convolve(HALO, TOK - HALO)

    packed = routes[...]
    turned = jnp.concatenate([packed, jnp.zeros((LANES - 8, PAD_TOK), f32)], axis=0).T
    lanes_e = iota((TOK, E), 1).astype(f32)
    member = jnp.zeros((TOK, E), f32)
    weight = jnp.zeros((TOK, E), f32)
    for k in range(TOPK):
        hit = turned[:TOK, k : k + 1] == lanes_e
        member = jnp.where(hit, 1.0, member)
        weight = jnp.where(hit, turned[:TOK, TOPK + k : TOPK + k + 1], weight)
    before = (iota((TOK, TOK), 1) < iota((TOK, TOK), 0)).astype(f32).astype(bf16)
    place = jnp.dot(before, member.astype(bf16), preferred_element_type=f32)
    place = jnp.where(member > 0.0, place, -1.0).astype(bf16)
    weight_hi = weight.astype(bf16)
    weight_lo = (weight - weight_hi.astype(f32)).astype(bf16)
    for g in range(ROWS // LANES):
        spread_to = (iota((E, LANES), 1) // CAP + g * (LANES // CAP) == iota((E, LANES), 0)).astype(f32).astype(bf16)
        slots = jnp.dot(place, spread_to, preferred_element_type=f32)
        mine = slots == lax.rem(iota((TOK, LANES), 1), CAP).astype(f32)
        for part, held in ((weight_hi, mixer_hi), (weight_lo, mixer_lo)):
            wide = jnp.dot(part, spread_to, preferred_element_type=f32)
            held[:, g * LANES : (g + 1) * LANES] = jnp.where(mine, wide, 0.0).astype(bf16)

    tall_e = iota((E, TOK), 0).astype(f32)
    member = jnp.zeros((E, TOK), f32)
    for k in range(TOPK):
        member = jnp.where(packed[k : k + 1, :TOK] == tall_e, 1.0, member)
    after = (iota((TOK, TOK), 0) < iota((TOK, TOK), 1)).astype(f32).astype(bf16)
    place = jnp.dot(member.astype(bf16), after, preferred_element_type=f32)
    place = jnp.where(member > 0.0, place, -1.0)
    tall_c = iota((CAP, TOK), 0).astype(f32)
    for e in range(E):
        picker[e * CAP : (e + 1) * CAP, :] = (place[e : e + 1, :] == tall_c).astype(f32).astype(bf16)

    fetches[4].wait()
    columns = jnp.concatenate([mix_gain[...], jnp.zeros((LANES - SIDE * SIDE, LANES), f32)], axis=0).T
    for b in range(SIDE * SIDE):
        part = slice(b * LANES, (b + 1) * LANES)
        scaled_out[part, :] = (outw[part, :].astype(f32) * columns[:, b : b + 1]).astype(bf16)

    pl.semaphore_wait(barrier, E - 1 + len(mates))

    tail = copy_to(padded.at[pl.ds(TOK, HALO), :], halo, halo_send, halo_recv, {"sp": lax.rem(sp + 1, E)})
    tail.start()
    tail.wait()
    padded[:HALO, :] = jnp.where(sp > 0, halo[...], 0.0)
    conv[:HALO, :] = convolve(0, HALO)

    mean = jnp.mean(conv[...], axis=1, keepdims=True)
    centred = conv[...] - mean
    spread = jnp.sum(centred * centred, axis=1, keepdims=True)
    lane = iota((TOK, LANES), 1)
    both = jnp.where(lane == 0, mean, jnp.where(lane == 1, spread, 0.0))
    both = jnp.concatenate([both, jnp.zeros((PAD_TOK - TOK, LANES), f32)], axis=0).T[:8, :]
    gain_row = jnp.concatenate([norm_gain[...], norm_gain[...]], axis=1)
    message[...] = jnp.where(iota((8, PAD_TOK), 0) == 2, gain_row, both)
    me = y * SIDE + x
    for mate in mates:
        copy_to(message, stats.at[me], stat_send, stat_recv, mate).start()
    stats[me] = message[...]
    fetches[3].wait()
    most = stats.at[pl.ds(0, SIDE * SIDE - 1)]
    arrived = copy_to(most, most, stat_send, stat_recv, mates[0])
    arrived.wait_recv()
    means = stats[:, 0, :]
    gains[...] = stats[:, 2, :LANES]
    mean = jnp.mean(means, axis=0, keepdims=True)
    apart = means - mean
    var = (
        jnp.sum(stats[:, 1, :], axis=0, keepdims=True) + LANES * jnp.sum(apart * apart, axis=0, keepdims=True)
    ) / WIDE
    inverse = lax.rsqrt(var + epsilon)
    mean_t = jnp.broadcast_to(mean, (LANES, PAD_TOK)).T[:TOK, :]
    inverse_t = jnp.broadcast_to(inverse, (LANES, PAD_TOK)).T[:TOK, :]
    act = jax.nn.silu((conv[...] - mean_t) * inverse_t * chan_gain[...]).astype(bf16)

    for j in range(SIDE * SIDE // 2):
        pair = jnp.dot(
            act, pointw[:, 2 * j * LANES : 2 * (j + 1) * LANES], preferred_element_type=f32
        ).astype(bf16)
        for k in range(2):
            b = 2 * j + k
            mix_part[b // SIDE, b % SIDE, :, :] = pair[:, k * LANES : (k + 1) * LANES]
    mlands = (mland0, mland1, mland2, mland3)
    count = TOK // MIX_CHUNKS
    mreduces = [Reduce(plane, mix_part, c * count, count, mlands, mrs_send, mrs_recv, c) for c in range(MIX_CHUNKS)]
    mgathers = [Gather(plane, mix_rows, c * count, count, mag_send, mag_recv, c) for c in range(MIX_CHUNKS)]
    for step in range(4):
        for c in range(MIX_CHUNKS):
            mreduces[c].issue(step)
    for c in range(MIX_CHUNKS):
        for color in range(2):
            mix_rows[y, x, mreduces[c].rows(color), :] = mreduces[c].total(color).astype(bf16)
        mgathers[c].issue(0)
    for c in range(MIX_CHUNKS):
        mgathers[c].issue(1)
    for c in range(MIX_CHUNKS):
        mgathers[c].arrived(1)
        mgathers[c].issue(2)
    for c in range(MIX_CHUNKS):
        mgathers[c].issue(3)
    for c in range(MIX_CHUNKS):
        mgathers[c].arrived(3)

    squares = jnp.zeros((TOK, LANES), f32)
    for b in range(SIDE * SIDE):
        block = mix_rows[b // SIDE, b % SIDE].astype(f32)
        squares = squares + block * block
    scale = lax.rsqrt(jnp.sum(squares, axis=1, keepdims=True) / WIDE + epsilon)
    left = jnp.concatenate([mix_rows[b // SIDE, b % SIDE] for b in range(SIDE * SIDE)], axis=1)
    branch = jnp.dot(left, scaled_out[...], preferred_element_type=f32) * scale
    fetches[5].wait()
    mid[...] = (resid[...].astype(f32) + branch).astype(bf16)
    picked = jnp.dot(picker[...], mid[...], preferred_element_type=f32).astype(bf16)
    outgoing[...] = picked.reshape(E, CAP, LANES)

    other = 1 - core
    for i, offset in enumerate(OFFSETS):
        chip = lax.rem(z - offset + CHIPS, CHIPS)
        spot = pl.ds(pl.multiple_of((2 * i + core) * CAP, CAP), CAP)
        for way in range(2):
            if i == 0 and way == 1:
                continue
            target = 2 * chip + (other if i == 0 else way)
            copy_to(
                outgoing.at[target],
                rows.at[y, x, spot, :],
                out_send,
                out_recv.at[2 * i // PERCHUNK],
                {"sp": target},
            ).start()
    own_place = pl.ds(pl.multiple_of(core * CAP, CAP), CAP)
    rows[y, x, own_place, :] = outgoing[sp]

    gathers = [Gather(plane, rows, c * CROWS, CROWS, ag_send, ag_recv, c) for c in range(CHUNKS)]
    lands = (land0, land1, land2, land3)
    reduces = [Reduce(plane, partial, c * CROWS, CROWS, lands, rs_send, rs_recv, c) for c in range(CHUNKS)]

    def begin(c):
        count = CROWS - (CAP if c == 0 else 0)
        landed = rows.at[y, x, pl.ds(c * CROWS, count), :]
        copy_to(landed, landed, out_send, out_recv.at[c], {"sp": lax.rem(sp + 1, E)}).wait_recv()
        gathers[c].issue(0)

    def compute(c):
        gathers[c].arrived(3)
        if c == 0:
            for fetch in fetches[6:]:
                fetch.wait()
        step = 32

        @pl.loop(0, CROWS // step)
        def _(i):
            at = pl.multiple_of(i * step, step)
            block = rows[:, :, pl.ds(c * CROWS + at, step), :].astype(f32)
            block = block.reshape(SIDE * SIDE, step, LANES)
            squares = jnp.sum(jnp.sum(block * block, axis=0), axis=1, keepdims=True)
            scale = lax.rsqrt(squares / WIDE + epsilon)
            scaled = block * scale[None] * gains[...][:, None, :]
            normed[:, pl.ds(at, step), :] = scaled.astype(bf16)

        left = jnp.concatenate([normed[b] for b in range(SIDE * SIDE)], axis=1)
        gate_pre = jnp.minimum(jnp.dot(left, gate[...], preferred_element_type=f32), clamp_limit)
        up_pre = jnp.clip(jnp.dot(left, up[...], preferred_element_type=f32), -clamp_limit, clamp_limit)
        hidden = (gate_pre * jax.nn.sigmoid(swish_slope * gate_pre) * (up_pre + 1.0)).astype(bf16)
        spot = pl.ds(c * CROWS, CROWS)
        for j in range(SIDE * SIDE // 2):
            pair = jnp.dot(
                hidden, down[:, 2 * j * LANES : 2 * (j + 1) * LANES], preferred_element_type=f32
            ).astype(bf16)
            for k in range(2):
                b = 2 * j + k
                partial[b // SIDE, b % SIDE, spot, :] = pair[:, k * LANES : (k + 1) * LANES]
        reduces[c].issue(0)

    def finish(c):
        half = CROWS // 2
        for color in range(2):
            total[pl.ds(c * CROWS + color * half, half), :] = reduces[c].total(color).astype(bf16)
        for p in range(c * PERCHUNK, (c + 1) * PERCHUNK):
            i, way = p // 2, p % 2
            if i == 0 and way == 1:
                continue
            chip = lax.rem(z + OFFSETS[i] + CHIPS, CHIPS)
            if i == 0:
                target = 2 * chip + other
                src = total.at[pl.ds(pl.multiple_of(other * CAP, CAP), CAP), :]
            else:
                target = 2 * chip + way
                src = total.at[pl.ds(p * CAP, CAP), :]
            copy_to(src, back.at[sp], back_send, back_recv, {"sp": target}).start()
        if c == 0:
            back[sp] = total[own_place, :]

    stages = [
        begin,
        lambda c: gathers[c].issue(1),
        lambda c: (gathers[c].arrived(1), gathers[c].issue(2)),
        lambda c: gathers[c].issue(3),
        compute,
        lambda c: reduces[c].issue(1),
        lambda c: reduces[c].issue(2),
        lambda c: reduces[c].issue(3),
        finish,
    ]
    for slot in range(CHUNKS + len(stages) - 1):
        for stage in (0, 1, 2, 3, 5, 6, 7, 8, 4):
            c = slot - stage
            if 0 <= c < CHUNKS:
                stages[stage](c)

    whole = back.at[pl.ds(0, E - 1)]
    copy_to(whole, whole, back_send, back_recv, {"sp": lax.rem(sp + 1, E)}).wait_recv()
    values = back[...].reshape(ROWS, LANES)
    routed = jnp.dot(mixer_hi[...], values, preferred_element_type=f32)
    routed = routed + jnp.dot(mixer_lo[...], values, preferred_element_type=f32)
    result[...] = (mid[...].astype(f32) + routed).astype(bf16)

    arrived.wait_send()
    sent = outgoing.at[pl.ds(0, E - 1)]
    copy_to(sent, sent, out_send, out_recv.at[0], {"sp": lax.rem(sp + 1, E)}).wait_send()
    sent = total.at[pl.ds(0, ROWS - CAP), :]
    copy_to(sent, sent, back_send, back_recv, {"sp": lax.rem(sp + 1, E)}).wait_send()
    for op in (*mreduces, *mgathers, *gathers, *reduces):
        op.sent()


def shards(
    resid,
    conv_value,
    conv_gate,
    depth_kernel,
    chan_gain,
    point_weight,
    mix_gain,
    out_weight,
    norm_gain,
    route_ids,
    route_weights,
    gate_experts,
    up_experts,
    down_experts,
):
    routes = jnp.concatenate([route_ids.T.astype(jnp.float32), route_weights.T], axis=0)
    routes = jnp.pad(routes, ((0, 0), (0, PAD_TOK - TOK)))
    vmem = pl.BlockSpec(memory_space=pltpu.VMEM)
    hbm = pl.BlockSpec(memory_space=pl.ANY)
    f32, bf16 = jnp.float32, jnp.bfloat16
    depth, hidden = gate_experts.shape[1], gate_experts.shape[2]
    sems = pltpu.SemaphoreType.DMA((CHUNKS, 2, 4, 2))
    msems = pltpu.SemaphoreType.DMA((MIX_CHUNKS, 2, 4, 2))
    one = pltpu.SemaphoreType.DMA
    fed = (conv_value, conv_gate, depth_kernel, resid, point_weight, out_weight)
    experts = (gate_experts, up_experts, down_experts)
    return pl.pallas_call(
        layer_kernel,
        out_shape=jax.ShapeDtypeStruct(resid.shape, bf16),
        in_specs=[hbm] * 9 + [vmem] * 4,
        out_specs=vmem,
        scratch_shapes=[
            *(pltpu.VMEM(a.shape, a.dtype) for a in fed),
            *(pltpu.VMEM(a.shape[1:], a.dtype) for a in experts),
            pltpu.VMEM((HALO + TOK, LANES), f32),
            pltpu.VMEM((HALO, LANES), f32),
            pltpu.VMEM((TOK, LANES), f32),
            pltpu.VMEM((8, PAD_TOK), f32),
            pltpu.VMEM((SIDE * SIDE, 8, PAD_TOK), f32),
            pltpu.VMEM((SIDE * SIDE, LANES), f32),
            pltpu.VMEM((depth, LANES), bf16),
            pltpu.VMEM((ROWS, TOK), bf16),
            pltpu.VMEM((TOK, ROWS), bf16),
            pltpu.VMEM((TOK, ROWS), bf16),
            pltpu.VMEM((TOK, LANES), bf16),
            pltpu.VMEM((E, CAP, LANES), bf16),
            pltpu.VMEM((SIDE, SIDE, TOK, LANES), bf16),
            pltpu.VMEM((SIDE, SIDE, TOK, LANES), bf16),
            *land_shapes(MIX_CHUNKS, TOK // MIX_CHUNKS),
            pltpu.VMEM((SIDE, SIDE, ROWS, LANES), bf16),
            pltpu.VMEM((SIDE * SIDE, CROWS, LANES), bf16),
            pltpu.VMEM((SIDE, SIDE, ROWS, LANES), bf16),
            *land_shapes(CHUNKS, CROWS),
            pltpu.VMEM((ROWS, LANES), bf16),
            pltpu.VMEM((E, CAP, LANES), bf16),
            one((9,)),
            one,
            one,
            one,
            one,
            msems,
            msems,
            msems,
            msems,
            sems,
            sems,
            sems,
            sems,
            one,
            one((CHUNKS,)),
            one,
            one,
        ],
        compiler_params=pltpu.CompilerParams(
            collective_id=1, has_side_effects=True, vmem_limit_bytes=48 * 1024 * 1024
        ),
        name="layer",
    )(
        conv_value,
        conv_gate,
        depth_kernel,
        resid,
        point_weight,
        out_weight,
        gate_experts,
        up_experts,
        down_experts,
        chan_gain.reshape(1, LANES),
        mix_gain.reshape(SIDE * SIDE, LANES),
        norm_gain.reshape(1, LANES),
        routes,
    )


def solution(mesh):
    split = Mesh(mesh.devices.reshape(mesh.shape["sp"], 4, 4), ("sp", "tp_0", "tp_1"))
    return jax.shard_map(
        shards,
        mesh=split,
        in_specs=(
            P("sp", TP),
            P("sp", TP),
            P("sp", TP),
            P(None, TP),
            P(TP),
            P(TP, None),
            P(),
            P(None, TP),
            P(TP),
            P("sp", None),
            P("sp", None),
            P("sp", None, TP),
            P("sp", None, TP),
            P("sp", TP, None),
        ),
        out_specs=P("sp", TP),
        check_vma=False,
    )
```

```python
import jax
import jax.numpy as jnp
from jax import lax
from jax.experimental import pallas as pl
from jax.experimental.pallas import tpu as pltpu
from jax.sharding import Mesh
from jax.sharding import PartitionSpec as P

E = 32
TOPK = 4
CAP = 32
TP = ("tp_0", "tp_1")
MESH = pl.DeviceIdType.MESH

epsilon = 1e-05
clamp_limit = 7.0
swish_slope = 1.702

SIDE = 4
CHIPS = 16
LANES = 128
ROWS = E * CAP
CHUNKS = 4
CROWS = ROWS // CHUNKS
PERCHUNK = CROWS // CAP
OFFSETS = [0, 1, -1, 2, -2, 3, -3, 4, -4, 5, -5, 6, -6, 7, -7, 8]


class Plane:
    def __init__(self, y, x):
        self.pos = (y, x)
        self.axes = ("tp_0", "tp_1")

    def neighbour(self, dim, step):
        return {self.axes[dim]: lax.rem(self.pos[dim] + step + SIDE, SIDE)}

    def at(self, dim, step):
        return lax.rem(self.pos[dim] + step + SIDE, SIDE)

    def line(self, ref, dim, index, rows):
        if dim == 0:
            return ref.at[index, :, rows, :]
        return ref.at[:, index, rows, :]

    def one(self, ref, dim, index, rows):
        if dim == 0:
            return ref.at[index, self.pos[1], rows, :]
        return ref.at[self.pos[0], index, rows, :]


def copy_to(src, dst, send, recv, device):
    return pltpu.make_async_remote_copy(
        src_ref=src, dst_ref=dst, send_sem=send, recv_sem=recv, device_id=device, device_id_type=MESH
    )


class Gather:
    def __init__(self, plane, buf, base, count, send, recv, chunk):
        self.plane, self.buf, self.chunk = plane, buf, chunk
        self.send, self.recv = send, recv
        self.half = count // 2
        self.quarter = count // 4
        self.base = base
        self.pending = {}

    def rows(self, color):
        start = self.base + color * self.half
        return pl.ds(start, self.half)

    def part(self, color, which):
        start = self.base + color * self.half + which * self.quarter
        return pl.ds(start, self.quarter)

    def go(self, color, step, way, src, dst, device):
        sem = (self.chunk, color, step, way)
        op = copy_to(src, dst, self.send.at[sem], self.recv.at[sem], device)
        op.start()
        self.pending[(color, step, way)] = op

    def issue(self, step):
        plane = self.plane
        for color in range(2):
            near = 1 - color
            far = color
            dim = near if step < 2 else far
            view = plane.one if step < 2 else plane.line
            ahead, behind = plane.neighbour(dim, 1), plane.neighbour(dim, -1)
            if step % 2 == 0:
                block = view(self.buf, dim, plane.pos[dim], self.rows(color))
                self.go(color, step, 0, block, block, ahead)
                self.go(color, step, 1, block, block, behind)
            else:
                self.pending[(color, step - 1, 0)].wait_recv()
                block = view(self.buf, dim, plane.at(dim, -1), self.part(color, 0))
                self.go(color, step, 0, block, block, ahead)
                self.pending[(color, step - 1, 1)].wait_recv()
                block = view(self.buf, dim, plane.at(dim, 1), self.part(color, 1))
                self.go(color, step, 1, block, block, behind)

    def arrived(self, step):
        for color in range(2):
            for way in range(2):
                self.pending[(color, step, way)].wait_recv()

    def sent(self):
        for op in self.pending.values():
            op.wait_send()


class Reduce:
    def __init__(self, plane, buf, base, count, lands, send, recv, chunk):
        self.plane, self.buf, self.chunk = plane, buf, chunk
        self.send, self.recv = send, recv
        self.half = count // 2
        self.quarter = count // 4
        self.base = base
        self.lands = lands
        self.pending = {}

    def rows(self, color):
        return pl.ds(self.base + color * self.half, self.half)

    def part(self, color, which):
        return pl.ds(self.base + color * self.half + which * self.quarter, self.quarter)

    def go(self, color, step, way, src, device):
        sem = (self.chunk, color, step, way)
        dst = self.lands[step].at[self.chunk, color, way]
        op = copy_to(src, dst, self.send.at[sem], self.recv.at[sem], device)
        op.start()
        self.pending[(color, step, way)] = op

    def land(self, color, step, way):
        self.pending[(color, step, way)].wait_recv()
        return self.lands[step].at[self.chunk, color, way]

    def issue(self, step):
        plane = self.plane
        for color in range(2):
            near = 1 - color
            far = color
            dim = far if step < 2 else near
            view = plane.line if step < 2 else plane.one
            ahead, behind = plane.neighbour(dim, 1), plane.neighbour(dim, -1)
            if step == 2:
                self.fold(color)
            if step % 2 == 0:
                opposite = plane.at(dim, 2)
                self.go(color, step, 0, view(self.buf, dim, opposite, self.part(color, 0)), ahead)
                self.go(color, step, 1, view(self.buf, dim, opposite, self.part(color, 1)), behind)
            else:
                for way, (shift, device) in enumerate(((1, ahead), (-1, behind))):
                    landed = self.land(color, step - 1, way)
                    target = view(self.buf, dim, plane.at(dim, shift), self.part(color, way))
                    target[...] = (target[...].astype(jnp.float32) + landed[...].astype(jnp.float32)).astype(
                        jnp.bfloat16
                    )
                    whole = view(self.buf, dim, plane.at(dim, shift), self.rows(color))
                    self.go(color, step, way, whole, device)

    def fold(self, color):
        plane = self.plane
        far = color
        own = plane.line(self.buf, far, plane.pos[far], self.rows(color))
        first, second = self.land(color, 1, 0), self.land(color, 1, 1)
        own[...] = (
            own[...].astype(jnp.float32) + first[...].astype(jnp.float32) + second[...].astype(jnp.float32)
        ).astype(jnp.bfloat16)

    def total(self, color):
        plane = self.plane
        near = 1 - color
        own = plane.one(self.buf, near, plane.pos[near], self.rows(color))
        first, second = self.land(color, 3, 0), self.land(color, 3, 1)
        return own[...].astype(jnp.float32) + first[...].astype(jnp.float32) + second[...].astype(jnp.float32)

    def sent(self):
        for op in self.pending.values():
            op.wait_send()


MIX_CHUNKS = 1
TOK = 192
HALO = 32
PAD_TOK = 256
TAPS = 31
WIDE = SIDE * SIDE * LANES


def land_shapes(chunks, count):
    half, quarter = count // 2, count // 4
    return [
        pltpu.VMEM((chunks, 2, 2, SIDE, quarter, LANES), jnp.bfloat16),
        pltpu.VMEM((chunks, 2, 2, SIDE, half, LANES), jnp.bfloat16),
        pltpu.VMEM((chunks, 2, 2, quarter, LANES), jnp.bfloat16),
        pltpu.VMEM((chunks, 2, 2, half, LANES), jnp.bfloat16),
    ]


def iota(shape, dim):
    return lax.broadcasted_iota(jnp.int32, shape, dim)


def layer_kernel(
    value_hbm,
    gating_hbm,
    taps_hbm,
    resid_hbm,
    point_hbm,
    outw_hbm,
    gate_hbm,
    up_hbm,
    down_hbm,
    chan_gain,
    mix_gain,
    norm_gain,
    routes,
    result,
    value,
    gating,
    taps,
    resid,
    pointw,
    outw,
    gate,
    up,
    down,
    padded,
    halo,
    conv,
    message,
    stats,
    gains,
    scaled_out,
    picker,
    mixer_hi,
    mixer_lo,
    mid,
    outgoing,
    mix_part,
    mix_rows,
    mland0,
    mland1,
    mland2,
    mland3,
    rows,
    normed,
    partial,
    land0,
    land1,
    land2,
    land3,
    total,
    back,
    fetch_sem,
    round_sem,
    halo_send,
    halo_recv,
    stat_send,
    stat_recv,
    mag_send,
    mag_recv,
    mrs_send,
    mrs_recv,
    ag_send,
    ag_recv,
    rs_send,
    rs_recv,
    out_send,
    out_recv,
    back_send,
    back_recv,
):
    f32, bf16 = jnp.float32, jnp.bfloat16
    sp = lax.axis_index("sp")
    y, x = lax.axis_index("tp_0"), lax.axis_index("tp_1")
    z, core = sp // 2, lax.rem(sp, 2)
    plane = Plane(y, x)

    barrier = pltpu.get_barrier_semaphore()

    mates = []
    for dy in range(SIDE):
        for dx in range(SIDE):
            if dy or dx:
                mates.append({"tp_0": lax.rem(y + dy, SIDE), "tp_1": lax.rem(x + dx, SIDE)})
    close = [{"sp": lax.rem(sp + d + E, E)} for d in (1, -1, 2, -2)]
    for mate in mates + close:
        pl.semaphore_signal(barrier, inc=1, device_id=mate, device_id_type=MESH)

    fetches = []
    for i, (src, dst) in enumerate(
        (
            (value_hbm, value),
            (gating_hbm, gating),
            (taps_hbm, taps),
            (point_hbm, pointw),
            (outw_hbm, outw),
            (resid_hbm, resid),
            (gate_hbm.at[0], gate),
            (up_hbm.at[0], up),
            (down_hbm.at[0], down),
        )
    ):
        fetch = pltpu.make_async_copy(src, dst, fetch_sem.at[i])
        fetch.start()
        fetches.append(fetch)

    def mixer_table():
        packed = routes[...]
        turned = jnp.concatenate([packed, jnp.zeros((LANES - 8, PAD_TOK), f32)], axis=0).T
        lanes_e = iota((TOK, E), 1).astype(f32)
        member = jnp.zeros((TOK, E), f32)
        weight = jnp.zeros((TOK, E), f32)
        for k in range(TOPK):
            hit = turned[:TOK, k : k + 1] == lanes_e
            member = jnp.where(hit, 1.0, member)
            weight = jnp.where(hit, turned[:TOK, TOPK + k : TOPK + k + 1], weight)
        before = (iota((TOK, TOK), 1) < iota((TOK, TOK), 0)).astype(f32).astype(bf16)
        place = jnp.dot(before, member.astype(bf16), preferred_element_type=f32)
        place = jnp.where(member > 0.0, place, -1.0).astype(bf16)
        weight_hi = weight.astype(bf16)
        weight_lo = (weight - weight_hi.astype(f32)).astype(bf16)
        for g in range(ROWS // LANES):
            spread_to = (iota((E, LANES), 1) // CAP + g * (LANES // CAP) == iota((E, LANES), 0)).astype(f32).astype(bf16)
            slots = jnp.dot(place, spread_to, preferred_element_type=f32)
            mine = slots == lax.rem(iota((TOK, LANES), 1), CAP).astype(f32)
            for part, held in ((weight_hi, mixer_hi), (weight_lo, mixer_lo)):
                wide = jnp.dot(part, spread_to, preferred_element_type=f32)
                held[:, g * LANES : (g + 1) * LANES] = jnp.where(mine, wide, 0.0).astype(bf16)

    def picker_table():
        packed = routes[...]
        tall_e = iota((E, TOK), 0).astype(f32)
        member = jnp.zeros((E, TOK), f32)
        for k in range(TOPK):
            member = jnp.where(packed[k : k + 1, :TOK] == tall_e, 1.0, member)
        after = (iota((TOK, TOK), 0) < iota((TOK, TOK), 1)).astype(f32).astype(bf16)
        place = jnp.dot(member.astype(bf16), after, preferred_element_type=f32)
        place = jnp.where(member > 0.0, place, -1.0)
        tall_c = iota((CAP, TOK), 0).astype(f32)
        for e in range(E):
            picker[e * CAP : (e + 1) * CAP, :] = (place[e : e + 1, :] == tall_c).astype(f32).astype(bf16)

    def scale_out():
        fetches[4].wait()
        columns = jnp.concatenate([mix_gain[...], jnp.zeros((LANES - SIDE * SIDE, LANES), f32)], axis=0).T
        for b in range(SIDE * SIDE):
            part = slice(b * LANES, (b + 1) * LANES)
            scaled_out[part, :] = (outw[part, :].astype(f32) * columns[:, b : b + 1]).astype(bf16)

    for i in range(3):
        fetches[i].wait()
    unit = value[...].astype(f32) * jax.nn.sigmoid(gating[...].astype(f32))
    padded[HALO:, :] = unit.astype(bf16).astype(f32)

    def convolve(first, count):
        acc = jnp.zeros((count, LANES), f32)
        for tap in range(TAPS):
            start = first + HALO - (TAPS - 1) + tap
            acc = acc + padded[start : start + count, :] * taps[tap : tap + 1, :]
        return acc

    conv[HALO:, :] = convolve(HALO, TOK - HALO)

    pl.semaphore_wait(barrier, len(mates) + len(close))

    def hear(r):
        pl.semaphore_wait(round_sem.at[r], 2)

    def tell(r):
        for d in (2 ** (r + 1), -(2 ** (r + 1))):
            pl.semaphore_signal(
                round_sem.at[r], inc=1, device_id={"sp": lax.rem(sp + d + E, E)}, device_id_type=MESH
            )

    tell(0)

    tail = copy_to(padded.at[pl.ds(TOK, HALO), :], halo, halo_send, halo_recv, {"sp": lax.rem(sp + 1, E)})
    tail.start()
    tail.wait()
    hear(0)
    tell(1)
    padded[:HALO, :] = jnp.where(sp > 0, halo[...], 0.0)
    conv[:HALO, :] = convolve(0, HALO)

    mean = jnp.mean(conv[...], axis=1, keepdims=True)
    centred = conv[...] - mean
    spread = jnp.sum(centred * centred, axis=1, keepdims=True)
    lane = iota((TOK, LANES), 1)
    both = jnp.where(lane == 0, mean, jnp.where(lane == 1, spread, 0.0))
    both = jnp.concatenate([both, jnp.zeros((PAD_TOK - TOK, LANES), f32)], axis=0).T[:8, :]
    gain_row = jnp.concatenate([norm_gain[...], norm_gain[...]], axis=1)
    message[...] = jnp.where(iota((8, PAD_TOK), 0) == 2, gain_row, both)
    me = y * SIDE + x
    for mate in mates:
        copy_to(message, stats.at[me], stat_send, stat_recv, mate).start()
    stats[me] = message[...]
    mixer_table()
    hear(1)
    tell(2)
    fetches[3].wait()
    most = stats.at[pl.ds(0, SIDE * SIDE - 1)]
    arrived = copy_to(most, most, stat_send, stat_recv, mates[0])
    arrived.wait_recv()
    means = stats[:, 0, :]
    gains[...] = stats[:, 2, :LANES]
    mean = jnp.mean(means, axis=0, keepdims=True)
    apart = means - mean
    var = (
        jnp.sum(stats[:, 1, :], axis=0, keepdims=True) + LANES * jnp.sum(apart * apart, axis=0, keepdims=True)
    ) / WIDE
    inverse = lax.rsqrt(var + epsilon)
    mean_t = jnp.broadcast_to(mean, (LANES, PAD_TOK)).T[:TOK, :]
    inverse_t = jnp.broadcast_to(inverse, (LANES, PAD_TOK)).T[:TOK, :]
    act = jax.nn.silu((conv[...] - mean_t) * inverse_t * chan_gain[...]).astype(bf16)

    for j in range(SIDE * SIDE // 2):
        pair = jnp.dot(
            act, pointw[:, 2 * j * LANES : 2 * (j + 1) * LANES], preferred_element_type=f32
        ).astype(bf16)
        for k in range(2):
            b = 2 * j + k
            mix_part[b // SIDE, b % SIDE, :, :] = pair[:, k * LANES : (k + 1) * LANES]
    mlands = (mland0, mland1, mland2, mland3)
    count = TOK // MIX_CHUNKS
    mreduces = [Reduce(plane, mix_part, c * count, count, mlands, mrs_send, mrs_recv, c) for c in range(MIX_CHUNKS)]
    mgathers = [Gather(plane, mix_rows, c * count, count, mag_send, mag_recv, c) for c in range(MIX_CHUNKS)]
    for step in range(4):
        for c in range(MIX_CHUNKS):
            mreduces[c].issue(step)
        if step == 0:
            picker_table()
        if step == 1:
            scale_out()
    for c in range(MIX_CHUNKS):
        for color in range(2):
            mix_rows[y, x, mreduces[c].rows(color), :] = mreduces[c].total(color).astype(bf16)
        mgathers[c].issue(0)
    for c in range(MIX_CHUNKS):
        mgathers[c].issue(1)
    for c in range(MIX_CHUNKS):
        mgathers[c].arrived(1)
        mgathers[c].issue(2)
    for c in range(MIX_CHUNKS):
        mgathers[c].issue(3)
    for c in range(MIX_CHUNKS):
        mgathers[c].arrived(3)

    squares = jnp.zeros((TOK, LANES), f32)
    for b in range(SIDE * SIDE):
        block = mix_rows[b // SIDE, b % SIDE].astype(f32)
        squares = squares + block * block
    scale = lax.rsqrt(jnp.sum(squares, axis=1, keepdims=True) / WIDE + epsilon)
    left = jnp.concatenate([mix_rows[b // SIDE, b % SIDE] for b in range(SIDE * SIDE)], axis=1)
    branch = jnp.dot(left, scaled_out[...], preferred_element_type=f32) * scale
    fetches[5].wait()
    mid[...] = (resid[...].astype(f32) + branch).astype(bf16)
    picked = jnp.dot(picker[...], mid[...], preferred_element_type=f32).astype(bf16)
    outgoing[...] = picked.reshape(E, CAP, LANES)

    hear(2)
    other = 1 - core
    for i, offset in enumerate(OFFSETS):
        chip = lax.rem(z - offset + CHIPS, CHIPS)
        spot = pl.ds(pl.multiple_of((2 * i + core) * CAP, CAP), CAP)
        for way in range(2):
            if i == 0 and way == 1:
                continue
            target = 2 * chip + (other if i == 0 else way)
            copy_to(
                outgoing.at[target],
                rows.at[y, x, spot, :],
                out_send,
                out_recv.at[2 * i // PERCHUNK],
                {"sp": target},
            ).start()
    own_place = pl.ds(pl.multiple_of(core * CAP, CAP), CAP)
    rows[y, x, own_place, :] = outgoing[sp]

    gathers = [Gather(plane, rows, c * CROWS, CROWS, ag_send, ag_recv, c) for c in range(CHUNKS)]
    lands = (land0, land1, land2, land3)
    reduces = [Reduce(plane, partial, c * CROWS, CROWS, lands, rs_send, rs_recv, c) for c in range(CHUNKS)]

    def begin(c):
        count = CROWS - (CAP if c == 0 else 0)
        landed = rows.at[y, x, pl.ds(c * CROWS, count), :]
        copy_to(landed, landed, out_send, out_recv.at[c], {"sp": lax.rem(sp + 1, E)}).wait_recv()
        gathers[c].issue(0)

    def compute(c):
        gathers[c].arrived(3)
        if c == 0:
            for fetch in fetches[6:]:
                fetch.wait()
        step = 32

        @pl.loop(0, CROWS // step)
        def _(i):
            at = pl.multiple_of(i * step, step)
            block = rows[:, :, pl.ds(c * CROWS + at, step), :].astype(f32)
            block = block.reshape(SIDE * SIDE, step, LANES)
            squares = jnp.sum(jnp.sum(block * block, axis=0), axis=1, keepdims=True)
            scale = lax.rsqrt(squares / WIDE + epsilon)
            scaled = block * scale[None] * gains[...][:, None, :]
            normed[:, pl.ds(at, step), :] = scaled.astype(bf16)

        left = jnp.concatenate([normed[b] for b in range(SIDE * SIDE)], axis=1)
        gate_pre = jnp.minimum(jnp.dot(left, gate[...], preferred_element_type=f32), clamp_limit)
        up_pre = jnp.clip(jnp.dot(left, up[...], preferred_element_type=f32), -clamp_limit, clamp_limit)
        hidden = (gate_pre * jax.nn.sigmoid(swish_slope * gate_pre) * (up_pre + 1.0)).astype(bf16)
        spot = pl.ds(c * CROWS, CROWS)
        for j in range(SIDE * SIDE // 2):
            pair = jnp.dot(
                hidden, down[:, 2 * j * LANES : 2 * (j + 1) * LANES], preferred_element_type=f32
            ).astype(bf16)
            for k in range(2):
                b = 2 * j + k
                partial[b // SIDE, b % SIDE, spot, :] = pair[:, k * LANES : (k + 1) * LANES]
        reduces[c].issue(0)

    def finish(c):
        half = CROWS // 2
        for color in range(2):
            total[pl.ds(c * CROWS + color * half, half), :] = reduces[c].total(color).astype(bf16)
        for p in range(c * PERCHUNK, (c + 1) * PERCHUNK):
            i, way = p // 2, p % 2
            if i == 0 and way == 1:
                continue
            chip = lax.rem(z + OFFSETS[i] + CHIPS, CHIPS)
            if i == 0:
                target = 2 * chip + other
                src = total.at[pl.ds(pl.multiple_of(other * CAP, CAP), CAP), :]
            else:
                target = 2 * chip + way
                src = total.at[pl.ds(p * CAP, CAP), :]
            copy_to(src, back.at[sp], back_send, back_recv, {"sp": target}).start()
        if c == 0:
            back[sp] = total[own_place, :]

    stages = [
        begin,
        lambda c: gathers[c].issue(1),
        lambda c: (gathers[c].arrived(1), gathers[c].issue(2)),
        lambda c: gathers[c].issue(3),
        compute,
        lambda c: reduces[c].issue(1),
        lambda c: reduces[c].issue(2),
        lambda c: reduces[c].issue(3),
        finish,
    ]
    for slot in range(CHUNKS + len(stages) - 1):
        for stage in (0, 1, 2, 3, 5, 6, 7, 8, 4):
            c = slot - stage
            if 0 <= c < CHUNKS:
                stages[stage](c)

    whole = back.at[pl.ds(0, E - 1)]
    copy_to(whole, whole, back_send, back_recv, {"sp": lax.rem(sp + 1, E)}).wait_recv()
    values = back[...].reshape(ROWS, LANES)
    routed = jnp.dot(mixer_hi[...], values, preferred_element_type=f32)
    routed = routed + jnp.dot(mixer_lo[...], values, preferred_element_type=f32)
    result[...] = (mid[...].astype(f32) + routed).astype(bf16)

    arrived.wait_send()
    sent = outgoing.at[pl.ds(0, E - 1)]
    copy_to(sent, sent, out_send, out_recv.at[0], {"sp": lax.rem(sp + 1, E)}).wait_send()
    sent = total.at[pl.ds(0, ROWS - CAP), :]
    copy_to(sent, sent, back_send, back_recv, {"sp": lax.rem(sp + 1, E)}).wait_send()
    for op in (*mreduces, *mgathers, *gathers, *reduces):
        op.sent()


def shards(
    resid,
    conv_value,
    conv_gate,
    depth_kernel,
    chan_gain,
    point_weight,
    mix_gain,
    out_weight,
    norm_gain,
    route_ids,
    route_weights,
    gate_experts,
    up_experts,
    down_experts,
):
    routes = jnp.concatenate([route_ids.T.astype(jnp.float32), route_weights.T], axis=0)
    routes = jnp.pad(routes, ((0, 0), (0, PAD_TOK - TOK)))
    vmem = pl.BlockSpec(memory_space=pltpu.VMEM)
    hbm = pl.BlockSpec(memory_space=pltpu.HBM)
    f32, bf16 = jnp.float32, jnp.bfloat16
    depth, hidden = gate_experts.shape[1], gate_experts.shape[2]
    sems = pltpu.SemaphoreType.DMA((CHUNKS, 2, 4, 2))
    msems = pltpu.SemaphoreType.DMA((MIX_CHUNKS, 2, 4, 2))
    one = pltpu.SemaphoreType.DMA
    fed = (conv_value, conv_gate, depth_kernel, resid, point_weight, out_weight)
    experts = (gate_experts, up_experts, down_experts)
    return pl.pallas_call(
        layer_kernel,
        out_shape=jax.ShapeDtypeStruct(resid.shape, bf16),
        in_specs=[hbm] * 9 + [vmem] * 4,
        out_specs=vmem,
        scratch_shapes=[
            *(pltpu.VMEM(a.shape, a.dtype) for a in fed),
            *(pltpu.VMEM(a.shape[1:], a.dtype) for a in experts),
            pltpu.VMEM((HALO + TOK, LANES), f32),
            pltpu.VMEM((HALO, LANES), f32),
            pltpu.VMEM((TOK, LANES), f32),
            pltpu.VMEM((8, PAD_TOK), f32),
            pltpu.VMEM((SIDE * SIDE, 8, PAD_TOK), f32),
            pltpu.VMEM((SIDE * SIDE, LANES), f32),
            pltpu.VMEM((depth, LANES), bf16),
            pltpu.VMEM((ROWS, TOK), bf16),
            pltpu.VMEM((TOK, ROWS), bf16),
            pltpu.VMEM((TOK, ROWS), bf16),
            pltpu.VMEM((TOK, LANES), bf16),
            pltpu.VMEM((E, CAP, LANES), bf16),
            pltpu.VMEM((SIDE, SIDE, TOK, LANES), bf16),
            pltpu.VMEM((SIDE, SIDE, TOK, LANES), bf16),
            *land_shapes(MIX_CHUNKS, TOK // MIX_CHUNKS),
            pltpu.VMEM((SIDE, SIDE, ROWS, LANES), bf16),
            pltpu.VMEM((SIDE * SIDE, CROWS, LANES), bf16),
            pltpu.VMEM((SIDE, SIDE, ROWS, LANES), bf16),
            *land_shapes(CHUNKS, CROWS),
            pltpu.VMEM((ROWS, LANES), bf16),
            pltpu.VMEM((E, CAP, LANES), bf16),
            one((9,)),
            pltpu.SemaphoreType.REGULAR((3,)),
            one,
            one,
            one,
            one,
            msems,
            msems,
            msems,
            msems,
            sems,
            sems,
            sems,
            sems,
            one,
            one((CHUNKS,)),
            one,
            one,
        ],
        compiler_params=pltpu.CompilerParams(
            collective_id=1, has_side_effects=True, vmem_limit_bytes=67043328
        ),
        name="layer",
    )(
        conv_value,
        conv_gate,
        depth_kernel,
        resid,
        point_weight,
        out_weight,
        gate_experts,
        up_experts,
        down_experts,
        chan_gain.reshape(1, LANES),
        mix_gain.reshape(SIDE * SIDE, LANES),
        norm_gain.reshape(1, LANES),
        routes,
    )


def solution(mesh):
    split = Mesh(mesh.devices.reshape(mesh.shape["sp"], 4, 4), ("sp", "tp_0", "tp_1"))
    return jax.shard_map(
        shards,
        mesh=split,
        in_specs=(
            P("sp", TP),
            P("sp", TP),
            P("sp", TP),
            P(None, TP),
            P(TP),
            P(TP, None),
            P(),
            P(None, TP),
            P(TP),
            P("sp", None),
            P("sp", None),
            P("sp", None, TP),
            P("sp", None, TP),
            P("sp", TP, None),
        ),
        out_specs=P("sp", TP),
        check_vma=False,
    )
```

```python
import jax
import jax.numpy as jnp
from jax import lax
from jax.experimental import pallas as pl
from jax.experimental.pallas import tpu as pltpu
from jax.sharding import Mesh
from jax.sharding import PartitionSpec as P

E = 32
TOPK = 4
CAP = 32
TP = ("tp_0", "tp_1")
MESH = pl.DeviceIdType.MESH

epsilon = 1e-05
clamp_limit = 7.0
swish_slope = 1.702

SIDE = 4
CHIPS = 16
LANES = 128
ROWS = E * CAP
CHUNKS = 4
CROWS = ROWS // CHUNKS
PERCHUNK = CROWS // CAP
OFFSETS = [0, 1, -1, 2, -4, 5, -5, 6, -6, 7, -7, 8, -2, 3, -3, 4]


class Plane:
    def __init__(self, y, x):
        self.pos = (y, x)
        self.axes = ("tp_0", "tp_1")

    def neighbour(self, dim, step):
        return {self.axes[dim]: lax.rem(self.pos[dim] + step + SIDE, SIDE)}

    def at(self, dim, step):
        return lax.rem(self.pos[dim] + step + SIDE, SIDE)

    def line(self, ref, dim, index, rows):
        if dim == 0:
            return ref.at[index, :, rows, :]
        return ref.at[:, index, rows, :]

    def one(self, ref, dim, index, rows):
        if dim == 0:
            return ref.at[index, self.pos[1], rows, :]
        return ref.at[self.pos[0], index, rows, :]


def copy_to(src, dst, send, recv, device):
    return pltpu.make_async_remote_copy(
        src_ref=src, dst_ref=dst, send_sem=send, recv_sem=recv, device_id=device, device_id_type=MESH
    )


class Gather:
    def __init__(self, plane, buf, base, count, send, recv, chunk, direct=False):
        self.plane, self.buf, self.chunk, self.direct = plane, buf, chunk, direct
        self.send, self.recv = send, recv
        self.half = count // 2
        self.quarter = count // 4
        self.base = base
        self.pending = {}

    def rows(self, color):
        start = self.base + color * self.half
        return pl.ds(start, self.half)

    def part(self, color, which):
        start = self.base + color * self.half + which * self.quarter
        return pl.ds(start, self.quarter)

    def go(self, color, step, way, src, dst, device):
        sem = (self.chunk, color, step, way)
        op = copy_to(src, dst, self.send.at[sem], self.recv.at[sem], device)
        op.start()
        self.pending[(color, step, way)] = op

    def issue(self, step):
        plane = self.plane
        for color in range(2):
            near = 1 - color
            far = color
            dim = near if step < 2 else far
            view = plane.one if step < 2 else plane.line
            ahead, behind = plane.neighbour(dim, 1), plane.neighbour(dim, -1)
            if step % 2 == 0:
                block = view(self.buf, dim, plane.pos[dim], self.rows(color))
                self.go(color, step, 0, block, block, ahead)
                self.go(color, step, 1, block, block, behind)
                if self.direct and step == 0:
                    self.go(color, 1, 0, block, block, plane.neighbour(dim, 2))
            elif self.direct and step == 1:
                for way in range(2):
                    self.pending[(color, 0, way)].wait_recv()
            else:
                self.pending[(color, step - 1, 0)].wait_recv()
                block = view(self.buf, dim, plane.at(dim, -1), self.part(color, 0))
                self.go(color, step, 0, block, block, ahead)
                self.pending[(color, step - 1, 1)].wait_recv()
                block = view(self.buf, dim, plane.at(dim, 1), self.part(color, 1))
                self.go(color, step, 1, block, block, behind)

    def arrived(self, step):
        for color in range(2):
            for way in range(2):
                if (color, step, way) in self.pending:
                    self.pending[(color, step, way)].wait_recv()

    def sent(self):
        for op in self.pending.values():
            op.wait_send()


class Reduce:
    def __init__(self, plane, buf, base, count, lands, send, recv, chunk, direct=False):
        self.plane, self.buf, self.chunk, self.direct = plane, buf, chunk, direct
        self.send, self.recv = send, recv
        self.half = count // 2
        self.quarter = count // 4
        self.base = base
        self.lands = lands
        self.pending = {}

    def rows(self, color):
        return pl.ds(self.base + color * self.half, self.half)

    def part(self, color, which):
        return pl.ds(self.base + color * self.half + which * self.quarter, self.quarter)

    def go(self, color, step, way, src, device):
        sem = (self.chunk, color, step, way)
        dst = self.lands[step].at[self.chunk, color, way]
        op = copy_to(src, dst, self.send.at[sem], self.recv.at[sem], device)
        op.start()
        self.pending[(color, step, way)] = op

    def land(self, color, step, way):
        self.pending[(color, step, way)].wait_recv()
        return self.lands[step].at[self.chunk, color, way]

    def issue(self, step):
        plane = self.plane
        for color in range(2):
            near = 1 - color
            far = color
            dim = far if step < 2 else near
            view = plane.line if step < 2 else plane.one
            ahead, behind = plane.neighbour(dim, 1), plane.neighbour(dim, -1)
            if step == 2:
                self.fold(color)
            if self.direct and step >= 2:
                if step == 2:
                    shifts = ((3, 0, 1), (3, 1, -1), (2, 0, 2))
                    for slot, way, shift in shifts:
                        block = view(self.buf, dim, plane.at(dim, shift), self.rows(color))
                        self.go(color, slot, way, block, plane.neighbour(dim, shift))
            elif step % 2 == 0:
                opposite = plane.at(dim, 2)
                self.go(color, step, 0, view(self.buf, dim, opposite, self.part(color, 0)), ahead)
                self.go(color, step, 1, view(self.buf, dim, opposite, self.part(color, 1)), behind)
            else:
                for way, (shift, device) in enumerate(((1, ahead), (-1, behind))):
                    landed = self.land(color, step - 1, way)
                    target = view(self.buf, dim, plane.at(dim, shift), self.part(color, way))
                    target[...] = (target[...].astype(jnp.float32) + landed[...].astype(jnp.float32)).astype(
                        jnp.bfloat16
                    )
                    whole = view(self.buf, dim, plane.at(dim, shift), self.rows(color))
                    self.go(color, step, way, whole, device)

    def fold(self, color):
        plane = self.plane
        far = color
        own = plane.line(self.buf, far, plane.pos[far], self.rows(color))
        first, second = self.land(color, 1, 0), self.land(color, 1, 1)
        own[...] = (
            own[...].astype(jnp.float32) + first[...].astype(jnp.float32) + second[...].astype(jnp.float32)
        ).astype(jnp.bfloat16)

    def total(self, color):
        plane = self.plane
        near = 1 - color
        own = plane.one(self.buf, near, plane.pos[near], self.rows(color))
        first, second = self.land(color, 3, 0), self.land(color, 3, 1)
        value = own[...].astype(jnp.float32) + first[...].astype(jnp.float32) + second[...].astype(jnp.float32)
        if self.direct:
            value = value + self.land(color, 2, 0)[...].astype(jnp.float32)
        return value

    def sent(self):
        for op in self.pending.values():
            op.wait_send()


MIX_CHUNKS = 3
TOK = 192
HALO = 32
PAD_TOK = 256
TAPS = 31
WIDE = SIDE * SIDE * LANES


def land_shapes(chunks, count, direct=False):
    half, quarter = count // 2, count // 4
    return [
        pltpu.VMEM((chunks, 2, 2, SIDE, quarter, LANES), jnp.bfloat16),
        pltpu.VMEM((chunks, 2, 2, SIDE, half, LANES), jnp.bfloat16),
        pltpu.VMEM((chunks, 2, 2, half if direct else quarter, LANES), jnp.bfloat16),
        pltpu.VMEM((chunks, 2, 2, half, LANES), jnp.bfloat16),
    ]


def iota(shape, dim):
    return lax.broadcasted_iota(jnp.int32, shape, dim)


def layer_kernel(
    value_hbm,
    gating_hbm,
    taps_hbm,
    resid_hbm,
    point_hbm,
    outw_hbm,
    gate_hbm,
    up_hbm,
    down_hbm,
    chan_hbm,
    mix_hbm,
    norm_hbm,
    ids_hbm,
    weights_hbm,
    result,
    value,
    gating,
    taps,
    resid,
    pointw,
    outw,
    gate,
    up,
    down,
    chan_gain,
    mix_gain,
    norm_gain,
    ids,
    weights,
    padded,
    halo,
    conv,
    message,
    stats,
    gains,
    scaled_out,
    picker,
    mixer_hi,
    mixer_lo,
    mid,
    outgoing,
    mix_part,
    mix_rows,
    mland0,
    mland1,
    mland2,
    mland3,
    rows,
    normed,
    partial,
    land0,
    land1,
    land2,
    land3,
    total,
    back,
    fetch_sem,
    round_sem,
    halo_send,
    halo_recv,
    stat_send,
    stat_recv,
    mag_send,
    mag_recv,
    mrs_send,
    mrs_recv,
    ag_send,
    ag_recv,
    rs_send,
    rs_recv,
    out_send,
    out_recv,
    back_send,
    back_recv,
):
    f32, bf16 = jnp.float32, jnp.bfloat16
    sp = lax.axis_index("sp")
    y, x = lax.axis_index("tp_0"), lax.axis_index("tp_1")
    z, core = sp // 2, lax.rem(sp, 2)
    plane = Plane(y, x)

    barrier = pltpu.get_barrier_semaphore()

    mates = []
    for dy in range(SIDE):
        for dx in range(SIDE):
            if dy or dx:
                mates.append({"tp_0": lax.rem(y + dy, SIDE), "tp_1": lax.rem(x + dx, SIDE)})
    close = [{"sp": lax.rem(sp + d + E, E)} for d in (1, -1, 2, -2)]
    for mate in mates + close:
        pl.semaphore_signal(barrier, inc=1, device_id=mate, device_id_type=MESH)

    fetches = []
    for i, (src, dst) in enumerate(
        (
            (value_hbm, value),
            (gating_hbm, gating),
            (taps_hbm, taps),
            (point_hbm, pointw),
            (outw_hbm, outw),
            (resid_hbm, resid),
            (gate_hbm.at[0], gate),
            (up_hbm.at[0], up),
            (down_hbm.at[0], down),
            (chan_hbm, chan_gain),
            (mix_hbm, mix_gain),
            (norm_hbm, norm_gain),
            (ids_hbm, ids),
            (weights_hbm, weights),
        )
    ):
        fetch = pltpu.make_async_copy(src, dst, fetch_sem.at[i])
        fetch.start()
        fetches.append(fetch)

    def mixer_table():
        packed = jnp.concatenate([ids[...].astype(f32), weights[...], jnp.zeros((LANES - 8, TOK), f32)], axis=0)
        turned = jnp.concatenate([packed, jnp.zeros((LANES, PAD_TOK - TOK), f32)], axis=1).T
        lanes_e = iota((TOK, E), 1).astype(f32)
        member = jnp.zeros((TOK, E), f32)
        weight = jnp.zeros((TOK, E), f32)
        for k in range(TOPK):
            hit = turned[:TOK, k : k + 1] == lanes_e
            member = jnp.where(hit, 1.0, member)
            weight = jnp.where(hit, turned[:TOK, TOPK + k : TOPK + k + 1], weight)
        before = (iota((TOK, TOK), 1) < iota((TOK, TOK), 0)).astype(f32).astype(bf16)
        place = jnp.dot(before, member.astype(bf16), preferred_element_type=f32)
        place = jnp.where(member > 0.0, place, -1.0).astype(bf16)
        weight_hi = weight.astype(bf16)
        weight_lo = (weight - weight_hi.astype(f32)).astype(bf16)
        for g in range(ROWS // LANES):
            spread_to = (iota((E, LANES), 1) // CAP + g * (LANES // CAP) == iota((E, LANES), 0)).astype(f32).astype(bf16)
            slots = jnp.dot(place, spread_to, preferred_element_type=f32)
            mine = slots == lax.rem(iota((TOK, LANES), 1), CAP).astype(f32)
            for part, held in ((weight_hi, mixer_hi), (weight_lo, mixer_lo)):
                wide = jnp.dot(part, spread_to, preferred_element_type=f32)
                held[:, g * LANES : (g + 1) * LANES] = jnp.where(mine, wide, 0.0).astype(bf16)

    def picker_table():
        packed = ids[...].astype(f32)
        tall_e = iota((E, TOK), 0).astype(f32)
        member = jnp.zeros((E, TOK), f32)
        for k in range(TOPK):
            member = jnp.where(packed[k : k + 1, :] == tall_e, 1.0, member)
        after = (iota((TOK, TOK), 0) < iota((TOK, TOK), 1)).astype(f32).astype(bf16)
        place = jnp.dot(member.astype(bf16), after, preferred_element_type=f32)
        place = jnp.where(member > 0.0, place, -1.0)
        tall_c = iota((CAP, TOK), 0).astype(f32)
        for e in range(E):
            picker[e * CAP : (e + 1) * CAP, :] = (place[e : e + 1, :] == tall_c).astype(f32).astype(bf16)

    def scale_out():
        fetches[4].wait()
        columns = jnp.concatenate([mix_gain[...], jnp.zeros((LANES - SIDE * SIDE, LANES), f32)], axis=0).T
        for b in range(SIDE * SIDE):
            part = slice(b * LANES, (b + 1) * LANES)
            scaled_out[part, :] = (outw[part, :].astype(f32) * columns[:, b : b + 1]).astype(bf16)

    for i in (0, 1, 2, 9, 10, 11, 12, 13):
        fetches[i].wait()
    unit = value[...].astype(f32) * jax.nn.sigmoid(gating[...].astype(f32))
    padded[HALO:, :] = unit.astype(bf16).astype(f32)

    def convolve(first, count):
        acc = jnp.zeros((count, LANES), f32)
        for tap in range(TAPS):
            start = first + HALO - (TAPS - 1) + tap
            acc = acc + padded[start : start + count, :] * taps[tap : tap + 1, :]
        return acc

    conv[HALO:, :] = convolve(HALO, TOK - HALO)

    pl.semaphore_wait(barrier, len(mates) + len(close))

    def hear(r):
        pl.semaphore_wait(round_sem.at[r], 2)

    def tell(r):
        for d in (2 ** (r + 1), -(2 ** (r + 1))):
            pl.semaphore_signal(
                round_sem.at[r], inc=1, device_id={"sp": lax.rem(sp + d + E, E)}, device_id_type=MESH
            )

    tell(0)

    tail = copy_to(padded.at[pl.ds(TOK, HALO), :], halo, halo_send, halo_recv, {"sp": lax.rem(sp + 1, E)})
    tail.start()
    tail.wait()
    hear(0)
    tell(1)
    padded[:HALO, :] = jnp.where(sp > 0, halo[...], 0.0)
    conv[:HALO, :] = convolve(0, HALO)

    mean = jnp.mean(conv[...], axis=1, keepdims=True)
    centred = conv[...] - mean
    spread = jnp.sum(centred * centred, axis=1, keepdims=True)
    lane = iota((TOK, LANES), 1)
    both = jnp.where(lane == 0, mean, jnp.where(lane == 1, spread, 0.0))
    both = jnp.concatenate([both, jnp.zeros((PAD_TOK - TOK, LANES), f32)], axis=0).T[:4, :]
    gain_row = jnp.concatenate([norm_gain[...], norm_gain[...]], axis=1)
    message[...] = jnp.where(iota((4, PAD_TOK), 0) == 2, gain_row, both)
    me = y * SIDE + x
    for mate in mates:
        copy_to(message, stats.at[me], stat_send, stat_recv, mate).start()
    stats[me] = message[...]
    mixer_table()
    hear(1)
    tell(2)
    fetches[3].wait()
    most = stats.at[pl.ds(0, SIDE * SIDE - 1)]
    arrived = copy_to(most, most, stat_send, stat_recv, mates[0])
    arrived.wait_recv()
    means = stats[:, 0, :]
    gains[...] = stats[:, 2, :LANES]
    mean = jnp.mean(means, axis=0, keepdims=True)
    apart = means - mean
    var = (
        jnp.sum(stats[:, 1, :], axis=0, keepdims=True) + LANES * jnp.sum(apart * apart, axis=0, keepdims=True)
    ) / WIDE
    inverse = lax.rsqrt(var + epsilon)
    mean_t = jnp.broadcast_to(mean, (LANES, PAD_TOK)).T[:TOK, :]
    inverse_t = jnp.broadcast_to(inverse, (LANES, PAD_TOK)).T[:TOK, :]
    act = jax.nn.silu((conv[...] - mean_t) * inverse_t * chan_gain[...]).astype(bf16)

    for j in range(SIDE * SIDE // 2):
        pair = jnp.dot(
            act, pointw[:, 2 * j * LANES : 2 * (j + 1) * LANES], preferred_element_type=f32
        ).astype(bf16)
        for k in range(2):
            b = 2 * j + k
            mix_part[b // SIDE, b % SIDE, :, :] = pair[:, k * LANES : (k + 1) * LANES]
    mlands = (mland0, mland1, mland2, mland3)
    count = TOK // MIX_CHUNKS
    mreduces = [Reduce(plane, mix_part, c * count, count, mlands, mrs_send, mrs_recv, c, True) for c in range(MIX_CHUNKS)]
    mgathers = [Gather(plane, mix_rows, c * count, count, mag_send, mag_recv, c, True) for c in range(MIX_CHUNKS)]
    for step in range(4):
        for c in range(MIX_CHUNKS):
            mreduces[c].issue(step)
        if step == 0:
            picker_table()
        if step == 1:
            scale_out()
    for c in range(MIX_CHUNKS):
        for color in range(2):
            mix_rows[y, x, mreduces[c].rows(color), :] = mreduces[c].total(color).astype(bf16)
        mgathers[c].issue(0)
    for c in range(MIX_CHUNKS):
        mgathers[c].issue(1)
    for c in range(MIX_CHUNKS):
        mgathers[c].arrived(1)
        mgathers[c].issue(2)
    for c in range(MIX_CHUNKS):
        mgathers[c].issue(3)
    fetches[5].wait()
    for c in range(MIX_CHUNKS):
        mgathers[c].arrived(3)
        part = pl.ds(c * count, count)
        squares = jnp.zeros((count, LANES), f32)
        pieces = []
        for b in range(SIDE * SIDE):
            piece = mix_rows[b // SIDE, b % SIDE, part, :]
            pieces.append(piece)
            squares = squares + piece.astype(f32) * piece.astype(f32)
        scale = lax.rsqrt(jnp.sum(squares, axis=1, keepdims=True) / WIDE + epsilon)
        left = jnp.concatenate(pieces, axis=1)
        branch = jnp.dot(left, scaled_out[...], preferred_element_type=f32) * scale
        mid[part, :] = (resid[part, :].astype(f32) + branch).astype(bf16)
    picked = jnp.dot(picker[...], mid[...], preferred_element_type=f32).astype(bf16)
    outgoing[...] = picked.reshape(E, CAP, LANES)

    hear(2)
    other = 1 - core
    for i, offset in enumerate(OFFSETS):
        chip = lax.rem(z - offset + CHIPS, CHIPS)
        spot = pl.ds(pl.multiple_of((2 * i + core) * CAP, CAP), CAP)
        for way in range(2):
            if i == 0 and way == 1:
                continue
            target = 2 * chip + (other if i == 0 else way)
            copy_to(
                outgoing.at[target],
                rows.at[y, x, spot, :],
                out_send,
                out_recv.at[2 * i // PERCHUNK],
                {"sp": target},
            ).start()
    own_place = pl.ds(pl.multiple_of(core * CAP, CAP), CAP)
    rows[y, x, own_place, :] = outgoing[sp]

    gathers = [Gather(plane, rows, c * CROWS, CROWS, ag_send, ag_recv, c) for c in range(CHUNKS)]
    lands = (land0, land1, land2, land3)
    reduces = [Reduce(plane, partial, c * CROWS, CROWS, lands, rs_send, rs_recv, c) for c in range(CHUNKS)]

    def begin(c):
        count = CROWS - (CAP if c == 0 else 0)
        landed = rows.at[y, x, pl.ds(c * CROWS, count), :]
        copy_to(landed, landed, out_send, out_recv.at[c], {"sp": lax.rem(sp + 1, E)}).wait_recv()
        gathers[c].issue(0)

    def compute(c):
        gathers[c].arrived(3)
        if c == 0:
            for fetch in fetches[6:9]:
                fetch.wait()
        step = 32

        @pl.loop(0, CROWS // step)
        def _(i):
            at = pl.multiple_of(i * step, step)
            block = rows[:, :, pl.ds(c * CROWS + at, step), :].astype(f32)
            block = block.reshape(SIDE * SIDE, step, LANES)
            squares = jnp.sum(jnp.sum(block * block, axis=0), axis=1, keepdims=True)
            scale = lax.rsqrt(squares / WIDE + epsilon)
            scaled = block * scale[None] * gains[...][:, None, :]
            normed[:, pl.ds(at, step), :] = scaled.astype(bf16)

        left = jnp.concatenate([normed[b] for b in range(SIDE * SIDE)], axis=1)
        gate_pre = jnp.minimum(jnp.dot(left, gate[...], preferred_element_type=f32), clamp_limit)
        up_pre = jnp.clip(jnp.dot(left, up[...], preferred_element_type=f32), -clamp_limit, clamp_limit)
        hidden = (gate_pre * jax.nn.sigmoid(swish_slope * gate_pre) * (up_pre + 1.0)).astype(bf16)
        spot = pl.ds(c * CROWS, CROWS)
        for j in range(SIDE * SIDE // 2):
            pair = jnp.dot(
                hidden, down[:, 2 * j * LANES : 2 * (j + 1) * LANES], preferred_element_type=f32
            ).astype(bf16)
            for k in range(2):
                b = 2 * j + k
                partial[b // SIDE, b % SIDE, spot, :] = pair[:, k * LANES : (k + 1) * LANES]
        reduces[c].issue(0)

    def finish(c):
        half = CROWS // 2
        for color in range(2):
            total[pl.ds(c * CROWS + color * half, half), :] = reduces[c].total(color).astype(bf16)
        for p in range(c * PERCHUNK, (c + 1) * PERCHUNK):
            i, way = p // 2, p % 2
            if i == 0 and way == 1:
                continue
            chip = lax.rem(z + OFFSETS[i] + CHIPS, CHIPS)
            if i == 0:
                target = 2 * chip + other
                src = total.at[pl.ds(pl.multiple_of(other * CAP, CAP), CAP), :]
            else:
                target = 2 * chip + way
                src = total.at[pl.ds(p * CAP, CAP), :]
            copy_to(src, back.at[sp], back_send, back_recv, {"sp": target}).start()
        if c == 0:
            back[sp] = total[own_place, :]

    stages = [
        begin,
        lambda c: gathers[c].issue(1),
        lambda c: (gathers[c].arrived(1), gathers[c].issue(2)),
        lambda c: gathers[c].issue(3),
        compute,
        lambda c: reduces[c].issue(1),
        lambda c: reduces[c].issue(2),
        lambda c: reduces[c].issue(3),
        finish,
    ]
    for slot in range(CHUNKS + len(stages) - 1):
        for stage in range(len(stages)):
            c = slot - stage
            if 0 <= c < CHUNKS:
                stages[stage](c)

    whole = back.at[pl.ds(0, E - 1)]
    copy_to(whole, whole, back_send, back_recv, {"sp": lax.rem(sp + 1, E)}).wait_recv()
    values = back[...].reshape(ROWS, LANES)
    routed = jnp.dot(mixer_hi[...], values, preferred_element_type=f32)
    routed = routed + jnp.dot(mixer_lo[...], values, preferred_element_type=f32)
    result[...] = (mid[...].astype(f32) + routed).astype(bf16)

    arrived.wait_send()
    sent = outgoing.at[pl.ds(0, E - 1)]
    copy_to(sent, sent, out_send, out_recv.at[0], {"sp": lax.rem(sp + 1, E)}).wait_send()
    sent = total.at[pl.ds(0, ROWS - CAP), :]
    copy_to(sent, sent, back_send, back_recv, {"sp": lax.rem(sp + 1, E)}).wait_send()
    for op in (*mreduces, *mgathers, *gathers, *reduces):
        op.sent()


def shards(
    resid,
    conv_value,
    conv_gate,
    depth_kernel,
    chan_gain,
    point_weight,
    mix_gain,
    out_weight,
    norm_gain,
    route_ids,
    route_weights,
    gate_experts,
    up_experts,
    down_experts,
):
    vmem = pl.BlockSpec(memory_space=pltpu.VMEM)
    hbm = pl.BlockSpec(memory_space=pltpu.HBM)
    f32, bf16 = jnp.float32, jnp.bfloat16
    depth, hidden = gate_experts.shape[1], gate_experts.shape[2]
    sems = pltpu.SemaphoreType.DMA((CHUNKS, 2, 4, 2))
    msems = pltpu.SemaphoreType.DMA((MIX_CHUNKS, 2, 4, 2))
    one = pltpu.SemaphoreType.DMA
    fed = (conv_value, conv_gate, depth_kernel, resid, point_weight, out_weight)
    experts = (gate_experts, up_experts, down_experts)
    small = (
        chan_gain.reshape(1, LANES),
        mix_gain.reshape(SIDE * SIDE, LANES),
        norm_gain.reshape(1, LANES),
        route_ids.T,
        route_weights.T,
    )
    return pl.pallas_call(
        layer_kernel,
        out_shape=jax.ShapeDtypeStruct(resid.shape, bf16),
        in_specs=[hbm] * 14,
        out_specs=vmem,
        scratch_shapes=[
            *(pltpu.VMEM(a.shape, a.dtype) for a in fed),
            *(pltpu.VMEM(a.shape[1:], a.dtype) for a in experts),
            *(pltpu.VMEM(a.shape, a.dtype) for a in small),
            pltpu.VMEM((HALO + TOK, LANES), f32),
            pltpu.VMEM((HALO, LANES), f32),
            pltpu.VMEM((TOK, LANES), f32),
            pltpu.VMEM((4, PAD_TOK), f32),
            pltpu.VMEM((SIDE * SIDE, 4, PAD_TOK), f32),
            pltpu.VMEM((SIDE * SIDE, LANES), f32),
            pltpu.VMEM((depth, LANES), bf16),
            pltpu.VMEM((ROWS, TOK), bf16),
            pltpu.VMEM((TOK, ROWS), bf16),
            pltpu.VMEM((TOK, ROWS), bf16),
            pltpu.VMEM((TOK, LANES), bf16),
            pltpu.VMEM((E, CAP, LANES), bf16),
            pltpu.VMEM((SIDE, SIDE, TOK, LANES), bf16),
            pltpu.VMEM((SIDE, SIDE, TOK, LANES), bf16),
            *land_shapes(MIX_CHUNKS, TOK // MIX_CHUNKS, True),
            pltpu.VMEM((SIDE, SIDE, ROWS, LANES), bf16),
            pltpu.VMEM((SIDE * SIDE, CROWS, LANES), bf16),
            pltpu.VMEM((SIDE, SIDE, ROWS, LANES), bf16),
            *land_shapes(CHUNKS, CROWS),
            pltpu.VMEM((ROWS, LANES), bf16),
            pltpu.VMEM((E, CAP, LANES), bf16),
            one((14,)),
            pltpu.SemaphoreType.REGULAR((3,)),
            one,
            one,
            one,
            one,
            msems,
            msems,
            msems,
            msems,
            sems,
            sems,
            sems,
            sems,
            one,
            one((CHUNKS,)),
            one,
            one,
        ],
        compiler_params=pltpu.CompilerParams(
            collective_id=1, has_side_effects=True, vmem_limit_bytes=67043328
        ),
        name="layer",
    )(
        conv_value,
        conv_gate,
        depth_kernel,
        resid,
        point_weight,
        out_weight,
        gate_experts,
        up_experts,
        down_experts,
        *small,
    )


def solution(mesh):
    split = Mesh(mesh.devices.reshape(mesh.shape["sp"], 4, 4), ("sp", "tp_0", "tp_1"))
    return jax.shard_map(
        shards,
        mesh=split,
        in_specs=(
            P("sp", TP),
            P("sp", TP),
            P("sp", TP),
            P(None, TP),
            P(TP),
            P(TP, None),
            P(),
            P(None, TP),
            P(TP),
            P("sp", None),
            P("sp", None),
            P("sp", None, TP),
            P("sp", None, TP),
            P("sp", TP, None),
        ),
        out_specs=P("sp", TP),
        check_vma=False,
    )
```

```python
import jax
import jax.numpy as jnp
from jax import lax
from jax.experimental import pallas as pl
from jax.experimental.pallas import tpu as pltpu
from jax.sharding import Mesh
from jax.sharding import PartitionSpec as P

E = 32
TOPK = 4
CAP = 32
TP = ("tp_0", "tp_1")
MESH = pl.DeviceIdType.MESH

epsilon = 1e-05
clamp_limit = 7.0
swish_slope = 1.702

SIDE = 4
CHIPS = 16
LANES = 128
ROWS = E * CAP
CHUNKS = 4
CROWS = ROWS // CHUNKS
PERCHUNK = CROWS // CAP
OFFSETS = [0, 1, -1, 2, -4, 5, -5, 6, -6, 7, -7, 8, -2, 3, -3, 4]


class Plane:
    def __init__(self, y, x):
        self.pos = (y, x)
        self.axes = ("tp_0", "tp_1")

    def neighbour(self, dim, step):
        return {self.axes[dim]: lax.rem(self.pos[dim] + step + SIDE, SIDE)}

    def at(self, dim, step):
        return lax.rem(self.pos[dim] + step + SIDE, SIDE)

    def line(self, ref, dim, index, rows):
        if dim == 0:
            return ref.at[index, :, rows, :]
        return ref.at[:, index, rows, :]

    def one(self, ref, dim, index, rows):
        if dim == 0:
            return ref.at[index, self.pos[1], rows, :]
        return ref.at[self.pos[0], index, rows, :]


def copy_to(src, dst, send, recv, device):
    return pltpu.make_async_remote_copy(
        src_ref=src, dst_ref=dst, send_sem=send, recv_sem=recv, device_id=device, device_id_type=MESH
    )


class Gather:
    def __init__(self, plane, buf, base, count, send, recv, chunk, direct=False):
        self.plane, self.buf, self.chunk, self.direct = plane, buf, chunk, direct
        self.send, self.recv = send, recv
        self.half = count // 2
        self.quarter = count // 4
        self.base = base
        self.pending = {}

    def rows(self, color):
        start = self.base + color * self.half
        return pl.ds(start, self.half)

    def part(self, color, which):
        start = self.base + color * self.half + which * self.quarter
        return pl.ds(start, self.quarter)

    def go(self, color, step, way, src, dst, device):
        sem = (self.chunk, color, step, way)
        op = copy_to(src, dst, self.send.at[sem], self.recv.at[sem], device)
        op.start()
        self.pending[(color, step, way)] = op

    def issue(self, step):
        plane = self.plane
        for color in range(2):
            near = 1 - color
            far = color
            dim = near if step < 2 else far
            view = plane.one if step < 2 else plane.line
            ahead, behind = plane.neighbour(dim, 1), plane.neighbour(dim, -1)
            if step % 2 == 0:
                block = view(self.buf, dim, plane.pos[dim], self.rows(color))
                self.go(color, step, 0, block, block, ahead)
                self.go(color, step, 1, block, block, behind)
                if self.direct and step == 0:
                    self.go(color, 1, 0, block, block, plane.neighbour(dim, 2))
            elif self.direct and step == 1:
                for way in range(2):
                    self.pending[(color, 0, way)].wait_recv()
            else:
                self.pending[(color, step - 1, 0)].wait_recv()
                block = view(self.buf, dim, plane.at(dim, -1), self.part(color, 0))
                self.go(color, step, 0, block, block, ahead)
                self.pending[(color, step - 1, 1)].wait_recv()
                block = view(self.buf, dim, plane.at(dim, 1), self.part(color, 1))
                self.go(color, step, 1, block, block, behind)

    def arrived(self, step):
        for color in range(2):
            for way in range(2):
                if (color, step, way) in self.pending:
                    self.pending[(color, step, way)].wait_recv()

    def sent(self):
        for op in self.pending.values():
            op.wait_send()


class Reduce:
    def __init__(self, plane, buf, base, count, lands, send, recv, chunk, direct=False):
        self.plane, self.buf, self.chunk, self.direct = plane, buf, chunk, direct
        self.send, self.recv = send, recv
        self.half = count // 2
        self.quarter = count // 4
        self.base = base
        self.lands = lands
        self.pending = {}

    def rows(self, color):
        return pl.ds(self.base + color * self.half, self.half)

    def part(self, color, which):
        return pl.ds(self.base + color * self.half + which * self.quarter, self.quarter)

    def go(self, color, step, way, src, device):
        sem = (self.chunk, color, step, way)
        dst = self.lands[step].at[self.chunk, color, way]
        op = copy_to(src, dst, self.send.at[sem], self.recv.at[sem], device)
        op.start()
        self.pending[(color, step, way)] = op

    def land(self, color, step, way):
        self.pending[(color, step, way)].wait_recv()
        return self.lands[step].at[self.chunk, color, way]

    def issue(self, step):
        plane = self.plane
        for color in range(2):
            near = 1 - color
            far = color
            dim = far if step < 2 else near
            view = plane.line if step < 2 else plane.one
            ahead, behind = plane.neighbour(dim, 1), plane.neighbour(dim, -1)
            if step == 2:
                self.fold(color)
            if self.direct and step >= 2:
                if step == 2:
                    shifts = ((3, 0, 1), (3, 1, -1), (2, 0, 2))
                    for slot, way, shift in shifts:
                        block = view(self.buf, dim, plane.at(dim, shift), self.rows(color))
                        self.go(color, slot, way, block, plane.neighbour(dim, shift))
            elif step % 2 == 0:
                opposite = plane.at(dim, 2)
                self.go(color, step, 0, view(self.buf, dim, opposite, self.part(color, 0)), ahead)
                self.go(color, step, 1, view(self.buf, dim, opposite, self.part(color, 1)), behind)
            else:
                for way, (shift, device) in enumerate(((1, ahead), (-1, behind))):
                    landed = self.land(color, step - 1, way)
                    target = view(self.buf, dim, plane.at(dim, shift), self.part(color, way))
                    target[...] = (target[...].astype(jnp.float32) + landed[...].astype(jnp.float32)).astype(
                        jnp.bfloat16
                    )
                    whole = view(self.buf, dim, plane.at(dim, shift), self.rows(color))
                    self.go(color, step, way, whole, device)

    def fold(self, color):
        plane = self.plane
        far = color
        own = plane.line(self.buf, far, plane.pos[far], self.rows(color))
        first, second = self.land(color, 1, 0), self.land(color, 1, 1)
        own[...] = (
            own[...].astype(jnp.float32) + first[...].astype(jnp.float32) + second[...].astype(jnp.float32)
        ).astype(jnp.bfloat16)

    def total(self, color):
        plane = self.plane
        near = 1 - color
        own = plane.one(self.buf, near, plane.pos[near], self.rows(color))
        first, second = self.land(color, 3, 0), self.land(color, 3, 1)
        value = own[...].astype(jnp.float32) + first[...].astype(jnp.float32) + second[...].astype(jnp.float32)
        if self.direct:
            value = value + self.land(color, 2, 0)[...].astype(jnp.float32)
        return value

    def sent(self):
        for op in self.pending.values():
            op.wait_send()


MIX_CHUNKS = 3
TOK = 192
HALO = 32
PAD_TOK = 256
TAPS = 31
WIDE = SIDE * SIDE * LANES


def land_shapes(chunks, count, direct=False):
    half, quarter = count // 2, count // 4
    return [
        pltpu.VMEM((chunks, 2, 2, SIDE, quarter, LANES), jnp.bfloat16),
        pltpu.VMEM((chunks, 2, 2, SIDE, half, LANES), jnp.bfloat16),
        pltpu.VMEM((chunks, 2, 2, half if direct else quarter, LANES), jnp.bfloat16),
        pltpu.VMEM((chunks, 2, 2, half, LANES), jnp.bfloat16),
    ]


def iota(shape, dim):
    return lax.broadcasted_iota(jnp.int32, shape, dim)


def layer_kernel(
    value_hbm,
    gating_hbm,
    taps_hbm,
    resid_hbm,
    point_hbm,
    outw_hbm,
    gate_hbm,
    up_hbm,
    down_hbm,
    chan_hbm,
    mix_hbm,
    norm_hbm,
    ids_hbm,
    weights_hbm,
    result,
    value,
    gating,
    taps,
    resid,
    pointw,
    outw,
    gate,
    up,
    down,
    chan_gain,
    mix_gain,
    norm_gain,
    ids,
    weights,
    padded,
    halo,
    conv,
    message,
    stats,
    gains,
    scaled_out,
    picker,
    mixer_hi,
    mixer_lo,
    mid,
    outgoing,
    mix_part,
    mix_rows,
    mland0,
    mland1,
    mland2,
    mland3,
    rows,
    normed,
    partial,
    land0,
    land1,
    land2,
    land3,
    total,
    back,
    fetch_sem,
    round_sem,
    halo_send,
    halo_recv,
    stat_send,
    stat_recv,
    mag_send,
    mag_recv,
    mrs_send,
    mrs_recv,
    ag_send,
    ag_recv,
    rs_send,
    rs_recv,
    out_send,
    out_recv,
    back_send,
    back_recv,
):
    f32, bf16 = jnp.float32, jnp.bfloat16
    sp = lax.axis_index("sp")
    y, x = lax.axis_index("tp_0"), lax.axis_index("tp_1")
    z, core = sp // 2, lax.rem(sp, 2)
    plane = Plane(y, x)

    barrier = pltpu.get_barrier_semaphore()

    mates = []
    for dy in range(SIDE):
        for dx in range(SIDE):
            if dy or dx:
                mates.append({"tp_0": lax.rem(y + dy, SIDE), "tp_1": lax.rem(x + dx, SIDE)})
    close = [{"sp": lax.rem(sp + d + E, E)} for d in (1, -1, 2, -2)]
    for mate in mates + close:
        pl.semaphore_signal(barrier, inc=1, device_id=mate, device_id_type=MESH)

    fetches = []
    for i, (src, dst) in enumerate(
        (
            (value_hbm, value),
            (gating_hbm, gating),
            (taps_hbm, taps),
            (point_hbm, pointw),
            (outw_hbm, outw),
            (resid_hbm, resid),
            (gate_hbm.at[0], gate),
            (up_hbm.at[0], up),
            (down_hbm.at[0], down),
            (chan_hbm, chan_gain),
            (mix_hbm, mix_gain),
            (norm_hbm, norm_gain),
            (ids_hbm, ids),
            (weights_hbm, weights),
        )
    ):
        fetch = pltpu.make_async_copy(src, dst, fetch_sem.at[i])
        fetch.start()
        fetches.append(fetch)

    def mixer_table():
        packed = jnp.concatenate([ids[...].astype(f32), weights[...], jnp.zeros((LANES - 8, TOK), f32)], axis=0)
        turned = jnp.concatenate([packed, jnp.zeros((LANES, PAD_TOK - TOK), f32)], axis=1).T
        lanes_e = iota((TOK, E), 1).astype(f32)
        member = jnp.zeros((TOK, E), f32)
        weight = jnp.zeros((TOK, E), f32)
        for k in range(TOPK):
            hit = turned[:TOK, k : k + 1] == lanes_e
            member = jnp.where(hit, 1.0, member)
            weight = jnp.where(hit, turned[:TOK, TOPK + k : TOPK + k + 1], weight)
        before = (iota((TOK, TOK), 1) < iota((TOK, TOK), 0)).astype(f32).astype(bf16)
        place = jnp.dot(before, member.astype(bf16), preferred_element_type=f32)
        place = jnp.where(member > 0.0, place, -1.0).astype(bf16)
        weight_hi = weight.astype(bf16)
        weight_lo = (weight - weight_hi.astype(f32)).astype(bf16)
        for g in range(ROWS // LANES):
            spread_to = (iota((E, LANES), 1) // CAP + g * (LANES // CAP) == iota((E, LANES), 0)).astype(f32).astype(bf16)
            slots = jnp.dot(place, spread_to, preferred_element_type=f32)
            mine = slots == lax.rem(iota((TOK, LANES), 1), CAP).astype(f32)
            for part, held in ((weight_hi, mixer_hi), (weight_lo, mixer_lo)):
                wide = jnp.dot(part, spread_to, preferred_element_type=f32)
                held[:, g * LANES : (g + 1) * LANES] = jnp.where(mine, wide, 0.0).astype(bf16)

    def picker_table():
        packed = ids[...].astype(f32)
        tall_e = iota((E, TOK), 0).astype(f32)
        member = jnp.zeros((E, TOK), f32)
        for k in range(TOPK):
            member = jnp.where(packed[k : k + 1, :] == tall_e, 1.0, member)
        after = (iota((TOK, TOK), 0) < iota((TOK, TOK), 1)).astype(f32).astype(bf16)
        place = jnp.dot(member.astype(bf16), after, preferred_element_type=f32)
        place = jnp.where(member > 0.0, place, -1.0)
        tall_c = iota((CAP, TOK), 0).astype(f32)
        for e in range(E):
            picker[e * CAP : (e + 1) * CAP, :] = (place[e : e + 1, :] == tall_c).astype(f32).astype(bf16)

    def scale_out():
        fetches[4].wait()
        columns = jnp.concatenate([mix_gain[...], jnp.zeros((LANES - SIDE * SIDE, LANES), f32)], axis=0).T
        for b in range(SIDE * SIDE):
            part = slice(b * LANES, (b + 1) * LANES)
            scaled_out[part, :] = (outw[part, :].astype(f32) * columns[:, b : b + 1]).astype(bf16)

    for i in (0, 1, 2, 9, 10, 11, 12, 13):
        fetches[i].wait()
    unit = value[...].astype(f32) * jax.nn.sigmoid(gating[...].astype(f32))
    padded[HALO:, :] = unit.astype(bf16).astype(f32)

    def convolve(first, count):
        acc = jnp.zeros((count, LANES), f32)
        for tap in range(TAPS):
            start = first + HALO - (TAPS - 1) + tap
            acc = acc + padded[start : start + count, :] * taps[tap : tap + 1, :]
        return acc

    conv[HALO:, :] = convolve(HALO, TOK - HALO)

    pl.semaphore_wait(barrier, len(mates) + len(close))

    def hear(r):
        pl.semaphore_wait(round_sem.at[r], 2)

    def tell(r):
        for d in (2 ** (r + 1), -(2 ** (r + 1))):
            pl.semaphore_signal(
                round_sem.at[r], inc=1, device_id={"sp": lax.rem(sp + d + E, E)}, device_id_type=MESH
            )

    tell(0)

    tail = copy_to(padded.at[pl.ds(TOK, HALO), :], halo, halo_send, halo_recv, {"sp": lax.rem(sp + 1, E)})
    tail.start()
    tail.wait()
    hear(0)
    tell(1)
    padded[:HALO, :] = jnp.where(sp > 0, halo[...], 0.0)
    conv[:HALO, :] = convolve(0, HALO)

    mean = jnp.mean(conv[...], axis=1, keepdims=True)
    centred = conv[...] - mean
    spread = jnp.sum(centred * centred, axis=1, keepdims=True)
    lane = iota((TOK, LANES), 1)
    both = jnp.where(lane == 0, mean, jnp.where(lane == 1, spread, 0.0))
    both = jnp.concatenate([both, jnp.zeros((PAD_TOK - TOK, LANES), f32)], axis=0).T[:4, :]
    gain_row = jnp.concatenate([norm_gain[...], norm_gain[...]], axis=1)
    message[...] = jnp.where(iota((4, PAD_TOK), 0) == 2, gain_row, both)
    me = y * SIDE + x
    for mate in mates:
        copy_to(message, stats.at[me], stat_send, stat_recv, mate).start()
    stats[me] = message[...]
    mixer_table()
    hear(1)
    tell(2)
    fetches[3].wait()
    most = stats.at[pl.ds(0, SIDE * SIDE - 1)]
    arrived = copy_to(most, most, stat_send, stat_recv, mates[0])
    arrived.wait_recv()
    means = stats[:, 0, :]
    gains[...] = stats[:, 2, :LANES]
    mean = jnp.mean(means, axis=0, keepdims=True)
    apart = means - mean
    var = (
        jnp.sum(stats[:, 1, :], axis=0, keepdims=True) + LANES * jnp.sum(apart * apart, axis=0, keepdims=True)
    ) / WIDE
    inverse = lax.rsqrt(var + epsilon)
    mean_t = jnp.broadcast_to(mean, (LANES, PAD_TOK)).T[:TOK, :]
    inverse_t = jnp.broadcast_to(inverse, (LANES, PAD_TOK)).T[:TOK, :]
    act = jax.nn.silu((conv[...] - mean_t) * inverse_t * chan_gain[...]).astype(bf16)

    for j in range(SIDE * SIDE // 2):
        pair = jnp.dot(
            act, pointw[:, 2 * j * LANES : 2 * (j + 1) * LANES], preferred_element_type=f32
        ).astype(bf16)
        for k in range(2):
            b = 2 * j + k
            mix_part[b // SIDE, b % SIDE, :, :] = pair[:, k * LANES : (k + 1) * LANES]
    mlands = (mland0, mland1, mland2, mland3)
    count = TOK // MIX_CHUNKS
    mreduces = [Reduce(plane, mix_part, c * count, count, mlands, mrs_send, mrs_recv, c, True) for c in range(MIX_CHUNKS)]
    mgathers = [Gather(plane, mix_rows, c * count, count, mag_send, mag_recv, c, True) for c in range(MIX_CHUNKS)]
    for step in range(4):
        for c in range(MIX_CHUNKS):
            mreduces[c].issue(step)
        if step == 0:
            picker_table()
        if step == 1:
            scale_out()
    for c in range(MIX_CHUNKS):
        for color in range(2):
            mix_rows[y, x, mreduces[c].rows(color), :] = mreduces[c].total(color).astype(bf16)
        mgathers[c].issue(0)
    for c in range(MIX_CHUNKS):
        mgathers[c].issue(1)
    for c in range(MIX_CHUNKS):
        mgathers[c].arrived(1)
        mgathers[c].issue(2)
    for c in range(MIX_CHUNKS):
        mgathers[c].issue(3)
    fetches[5].wait()
    for c in range(MIX_CHUNKS):
        mgathers[c].arrived(3)
        part = pl.ds(c * count, count)
        squares = jnp.zeros((count, LANES), f32)
        pieces = []
        for b in range(SIDE * SIDE):
            piece = mix_rows[b // SIDE, b % SIDE, part, :]
            pieces.append(piece)
            squares = squares + piece.astype(f32) * piece.astype(f32)
        scale = lax.rsqrt(jnp.sum(squares, axis=1, keepdims=True) / WIDE + epsilon)
        left = jnp.concatenate(pieces, axis=1)
        branch = jnp.dot(left, scaled_out[...], preferred_element_type=f32) * scale
        mid[part, :] = (resid[part, :].astype(f32) + branch).astype(bf16)
    picked = jnp.dot(picker[...], mid[...], preferred_element_type=f32).astype(bf16)
    outgoing[...] = picked.reshape(E, CAP, LANES)

    hear(2)
    other = 1 - core
    for i, offset in enumerate(OFFSETS):
        chip = lax.rem(z - offset + CHIPS, CHIPS)
        spot = pl.ds(pl.multiple_of((2 * i + core) * CAP, CAP), CAP)
        for way in range(2):
            if i == 0 and way == 1:
                continue
            target = 2 * chip + (other if i == 0 else way)
            copy_to(
                outgoing.at[target],
                rows.at[y, x, spot, :],
                out_send,
                out_recv.at[2 * i // PERCHUNK],
                {"sp": target},
            ).start()
    own_place = pl.ds(pl.multiple_of(core * CAP, CAP), CAP)
    rows[y, x, own_place, :] = outgoing[sp]

    gathers = [Gather(plane, rows, c * CROWS, CROWS, ag_send, ag_recv, c) for c in range(CHUNKS)]
    lands = (land0, land1, land2, land3)
    reduces = [Reduce(plane, partial, c * CROWS, CROWS, lands, rs_send, rs_recv, c) for c in range(CHUNKS)]

    def begin(c):
        count = CROWS - (CAP if c == 0 else 0)
        landed = rows.at[y, x, pl.ds(c * CROWS, count), :]
        copy_to(landed, landed, out_send, out_recv.at[c], {"sp": lax.rem(sp + 1, E)}).wait_recv()
        gathers[c].issue(0)

    def compute(c):
        gathers[c].arrived(3)
        if c == 0:
            for fetch in fetches[6:9]:
                fetch.wait()
        step = 32

        @pl.loop(0, CROWS // step)
        def _(i):
            at = pl.multiple_of(i * step, step)
            block = rows[:, :, pl.ds(c * CROWS + at, step), :].astype(f32)
            block = block.reshape(SIDE * SIDE, step, LANES)
            squares = jnp.sum(jnp.sum(block * block, axis=0), axis=1, keepdims=True)
            scale = lax.rsqrt(squares / WIDE + epsilon)
            scaled = block * scale[None] * gains[...][:, None, :]
            normed[:, pl.ds(at, step), :] = scaled.astype(bf16)

        left = jnp.concatenate([normed[b] for b in range(SIDE * SIDE)], axis=1)
        gate_pre = jnp.minimum(jnp.dot(left, gate[...], preferred_element_type=f32), clamp_limit)
        up_pre = jnp.clip(jnp.dot(left, up[...], preferred_element_type=f32), -clamp_limit, clamp_limit)
        hidden = (gate_pre * jax.nn.sigmoid(swish_slope * gate_pre) * (up_pre + 1.0)).astype(bf16)
        spot = pl.ds(c * CROWS, CROWS)
        for j in range(SIDE * SIDE // 2):
            pair = jnp.dot(
                hidden, down[:, 2 * j * LANES : 2 * (j + 1) * LANES], preferred_element_type=f32
            ).astype(bf16)
            for k in range(2):
                b = 2 * j + k
                partial[b // SIDE, b % SIDE, spot, :] = pair[:, k * LANES : (k + 1) * LANES]
        reduces[c].issue(0)

    def finish(c):
        half = CROWS // 2
        for color in range(2):
            total[pl.ds(c * CROWS + color * half, half), :] = reduces[c].total(color).astype(bf16)
            first = c * PERCHUNK + color * PERCHUNK // 2
            for p in range(first, first + PERCHUNK // 2):
                i, way = p // 2, p % 2
                if i == 0 and way == 1:
                    continue
                chip = lax.rem(z + OFFSETS[i] + CHIPS, CHIPS)
                if i == 0:
                    target = 2 * chip + other
                    src = total.at[pl.ds(pl.multiple_of(other * CAP, CAP), CAP), :]
                else:
                    target = 2 * chip + way
                    src = total.at[pl.ds(p * CAP, CAP), :]
                copy_to(src, back.at[sp], back_send, back_recv, {"sp": target}).start()
        if c == 0:
            back[sp] = total[own_place, :]

    stages = [
        begin,
        lambda c: gathers[c].issue(1),
        lambda c: (gathers[c].arrived(1), gathers[c].issue(2)),
        lambda c: gathers[c].issue(3),
        compute,
        lambda c: reduces[c].issue(1),
        lambda c: reduces[c].issue(2),
        lambda c: reduces[c].issue(3),
        finish,
    ]
    for slot in range(CHUNKS + len(stages) - 1):
        for stage in range(len(stages)):
            c = slot - stage
            if 0 <= c < CHUNKS:
                stages[stage](c)

    whole = back.at[pl.ds(0, E - 1)]
    copy_to(whole, whole, back_send, back_recv, {"sp": lax.rem(sp + 1, E)}).wait_recv()
    values = back[...].reshape(ROWS, LANES)
    routed = jnp.dot(mixer_hi[...], values, preferred_element_type=f32)
    routed = routed + jnp.dot(mixer_lo[...], values, preferred_element_type=f32)
    result[...] = (mid[...].astype(f32) + routed).astype(bf16)

    arrived.wait_send()
    sent = outgoing.at[pl.ds(0, E - 1)]
    copy_to(sent, sent, out_send, out_recv.at[0], {"sp": lax.rem(sp + 1, E)}).wait_send()
    sent = total.at[pl.ds(0, ROWS - CAP), :]
    copy_to(sent, sent, back_send, back_recv, {"sp": lax.rem(sp + 1, E)}).wait_send()
    for op in (*mreduces, *mgathers, *gathers, *reduces):
        op.sent()


def shards(
    resid,
    conv_value,
    conv_gate,
    depth_kernel,
    chan_gain,
    point_weight,
    mix_gain,
    out_weight,
    norm_gain,
    route_ids,
    route_weights,
    gate_experts,
    up_experts,
    down_experts,
):
    vmem = pl.BlockSpec(memory_space=pltpu.VMEM)
    hbm = pl.BlockSpec(memory_space=pltpu.HBM)
    f32, bf16 = jnp.float32, jnp.bfloat16
    depth, hidden = gate_experts.shape[1], gate_experts.shape[2]
    sems = pltpu.SemaphoreType.DMA((CHUNKS, 2, 4, 2))
    msems = pltpu.SemaphoreType.DMA((MIX_CHUNKS, 2, 4, 2))
    one = pltpu.SemaphoreType.DMA
    fed = (conv_value, conv_gate, depth_kernel, resid, point_weight, out_weight)
    experts = (gate_experts, up_experts, down_experts)
    small = (
        chan_gain.reshape(1, LANES),
        mix_gain.reshape(SIDE * SIDE, LANES),
        norm_gain.reshape(1, LANES),
        route_ids.T,
        route_weights.T,
    )
    return pl.pallas_call(
        layer_kernel,
        out_shape=jax.ShapeDtypeStruct(resid.shape, bf16),
        in_specs=[hbm] * 14,
        out_specs=vmem,
        scratch_shapes=[
            *(pltpu.VMEM(a.shape, a.dtype) for a in fed),
            *(pltpu.VMEM(a.shape[1:], a.dtype) for a in experts),
            *(pltpu.VMEM(a.shape, a.dtype) for a in small),
            pltpu.VMEM((HALO + TOK, LANES), f32),
            pltpu.VMEM((HALO, LANES), f32),
            pltpu.VMEM((TOK, LANES), f32),
            pltpu.VMEM((4, PAD_TOK), f32),
            pltpu.VMEM((SIDE * SIDE, 4, PAD_TOK), f32),
            pltpu.VMEM((SIDE * SIDE, LANES), f32),
            pltpu.VMEM((depth, LANES), bf16),
            pltpu.VMEM((ROWS, TOK), bf16),
            pltpu.VMEM((TOK, ROWS), bf16),
            pltpu.VMEM((TOK, ROWS), bf16),
            pltpu.VMEM((TOK, LANES), bf16),
            pltpu.VMEM((E, CAP, LANES), bf16),
            pltpu.VMEM((SIDE, SIDE, TOK, LANES), bf16),
            pltpu.VMEM((SIDE, SIDE, TOK, LANES), bf16),
            *land_shapes(MIX_CHUNKS, TOK // MIX_CHUNKS, True),
            pltpu.VMEM((SIDE, SIDE, ROWS, LANES), bf16),
            pltpu.VMEM((SIDE * SIDE, CROWS, LANES), bf16),
            pltpu.VMEM((SIDE, SIDE, ROWS, LANES), bf16),
            *land_shapes(CHUNKS, CROWS),
            pltpu.VMEM((ROWS, LANES), bf16),
            pltpu.VMEM((E, CAP, LANES), bf16),
            one((14,)),
            pltpu.SemaphoreType.REGULAR((3,)),
            one,
            one,
            one,
            one,
            msems,
            msems,
            msems,
            msems,
            sems,
            sems,
            sems,
            sems,
            one,
            one((CHUNKS,)),
            one,
            one,
        ],
        compiler_params=pltpu.CompilerParams(
            collective_id=1, has_side_effects=True, vmem_limit_bytes=67043328
        ),
        name="layer",
    )(
        conv_value,
        conv_gate,
        depth_kernel,
        resid,
        point_weight,
        out_weight,
        gate_experts,
        up_experts,
        down_experts,
        *small,
    )


def solution(mesh):
    split = Mesh(mesh.devices.reshape(mesh.shape["sp"], 4, 4), ("sp", "tp_0", "tp_1"))
    return jax.shard_map(
        shards,
        mesh=split,
        in_specs=(
            P("sp", TP),
            P("sp", TP),
            P("sp", TP),
            P(None, TP),
            P(TP),
            P(TP, None),
            P(),
            P(None, TP),
            P(TP),
            P("sp", None),
            P("sp", None),
            P("sp", None, TP),
            P("sp", None, TP),
            P("sp", TP, None),
        ),
        out_specs=P("sp", TP),
        check_vma=False,
    )
```
